256 devices in a mesh: ep: 16 (over y, x), tp: 16 (over z, core).
Axes of the slice: x: 4, y: 4, z: 8, core: 2. Of those that a mesh axis runs over, the one named last changes fastest.
Arguments:
- pool_input: bfloat16 [32768, 1024], P('ep', 'tp'), may hold values from -6 to 6
- pool_gain: float32 [1024], P('tp'), may hold values from 0.1 to 1.9
- mix_weight: bfloat16 [1024, 2048], P('tp'), may hold values from -0.1875 to 0.1875
- moe_input: bfloat16 [65536, 2048], P(('ep', 'tp')), may hold values from -6 to 6
- moe_gain: float32 [2048], replicated, may hold values from 0.1 to 1.9
- expert_ids: int32 [65536, 2], P(('ep', 'tp')), may hold values from 0 to 15, as said below
- route_weight: float32 [65536, 2], P(('ep', 'tp')), may hold values from 0.2 to 1
- gate_weight: bfloat16 [16, 2048, 1024], P('ep', None, 'tp'), may hold values from -0.125 to 0.125
- up_weight: bfloat16 [16, 2048, 1024], P('ep', None, 'tp'), may hold values from -0.125 to 0.125
- down_weight: bfloat16 [16, 2048, 1024], P('ep', None, 'tp'), may hold values from -0.1875 to 0.1875
Outputs:
- mixed_out: bfloat16 [32768, 2048], P(('ep', 'tp'))
- moe_out: bfloat16 [65536, 2048], P(('ep', 'tp'))
The draws below stay inside these ranges and needn't reach their ends.
Inputs may be any that keep to these rules, and one draw needn't show every extreme that they name: `expert_ids`: each row names 2 different experts of one group of 4 consecutive experts. In each aligned block of 256 rows (the rows of one device) no expert is named by more than 48 rows, and some expert is named by exactly 48 rows.
All inputs are finite; a program needn't handle non-finite values.
Results may differ from the reference program's by a relative error of at most 0.012.
Values may be sent and summed in bfloat16 or wider, within the bound.
A program may use at most 128 MiB of HBM per device.

```python
import math
import jax
import jax.numpy as jnp
from jax import lax

D = 2048
PW = 1024
GROUP_CH = 256
FF = 1024
EXPERTS = 16
GROUP_EXP = 4
TOP = 2
ROWS_B = 256
CAP = 48
TOK_A = 32768
TOK_B = 65536


def block_routes(block_key):
    subkeys = jax.random.split(block_key, 5)
    remaining = ROWS_B - 2 * CAP
    share_base = remaining // 3
    spread = share_base // 4
    first_shift = jax.random.randint(subkeys[0], (), -spread, spread + 1)
    second_shift = jax.random.randint(subkeys[1], (), -spread, spread + 1)
    others = jnp.stack([share_base + first_shift, share_base + second_shift, remaining - 2 * share_base - first_shift - second_shift]).astype(jnp.int32)
    largest = jax.random.randint(subkeys[2], (), 0, 4)
    group_range = jnp.arange(4, dtype=jnp.int32)
    other_index = jnp.clip(group_range - (group_range > largest).astype(jnp.int32), 0, 2)
    quotas = jnp.where(group_range == largest, 2 * CAP, others[other_index]).astype(jnp.int32)
    group_ends = jnp.cumsum(quotas)
    position = jnp.arange(ROWS_B, dtype=jnp.int32)
    member = jnp.sum((position[:, None] >= group_ends[None, :]).astype(jnp.int32), axis=1)
    within = position - (group_ends - quotas)[member]
    leading = within % 4
    trailing = (within + 1 + within // 4 % 3) % 4
    relabel = jax.random.permutation(subkeys[3], 4).astype(jnp.int32)
    routes = jnp.stack([member * GROUP_EXP + relabel[leading], member * GROUP_EXP + relabel[trailing]], axis=1)
    return routes[jax.random.permutation(subkeys[4], ROWS_B)].astype(jnp.int32)


def draw_expert_ids(key, part):
    block_keys = jax.random.split(jax.random.fold_in(key, 7), TOK_B // ROWS_B)
    return jax.vmap(block_routes)(block_keys).reshape(TOK_B, 2)


def level_of(stream_key, shape, cuts, least, top_value):
    def one(dim, shards_of):
        heights = jax.random.uniform(jax.random.fold_in(jax.random.fold_in(stream_key, 6), dim), (shards_of,), jnp.float32, least / len(cuts), top_value / len(cuts))
        return jnp.repeat(jnp.exp(heights), shape[dim] // shards_of).reshape((-1,) + (1,) * (len(shape) - dim - 1))

    loudness = one(*cuts[0])
    for cut in cuts[1:]:
        loudness = loudness * one(*cut)
    return loudness


def normal_values(stream_key, dims, deviation, limit, cuts=(), kind=jnp.bfloat16):
    result = deviation * jax.random.normal(stream_key, dims, jnp.float32)
    if cuts:
        result = result * level_of(stream_key, dims, cuts, -0.22, 0.18)
    return jnp.clip(result, -limit, limit).astype(kind)


def setup_inputs(seed: int = 0) -> dict:
    key_of = jax.random.split(jax.random.key(seed), 11)
    pool_input = normal_values(key_of[0], (TOK_A, PW), 1.0, 6.0, ((0, 16), (1, 16)))
    pool_gain = jnp.clip(1.0 + 0.18 * jax.random.normal(key_of[1], (PW,), jnp.float32), 0.1, 1.9)
    mix_weight = normal_values(key_of[2], (PW, D), PW ** -0.5, 0.1875, ((0, 16),))
    moe_input = normal_values(key_of[3], (TOK_B, D), 1.0, 6.0, ((0, 256),))
    moe_gain = jnp.clip(1.0 + 0.18 * jax.random.normal(key_of[4], (D,), jnp.float32), 0.1, 1.9)
    expert_ids = draw_expert_ids(jax.random.fold_in(key_of[10], 71), 0)
    route_weight = jnp.clip(jnp.exp(math.log(1.0) - 1.609438 * jax.random.uniform(key_of[6], (TOK_B, TOP), jnp.float32) ** level_of(key_of[6], (TOK_B, TOP), ((0, 256),), -0.2, 0.2)), 0.2, 1.0)
    gate_weight = normal_values(key_of[7], (EXPERTS, D, FF), D ** -0.5, 0.125, ((0, 16), (2, 16)))
    up_weight = normal_values(key_of[8], (EXPERTS, D, FF), D ** -0.5, 0.125, ((0, 16), (2, 16)))
    down_weight = normal_values(key_of[9], (EXPERTS, D, FF), FF ** -0.5, 0.1875, ((0, 16), (2, 16)))
    return dict(pool_input=pool_input, pool_gain=pool_gain, mix_weight=mix_weight, moe_input=moe_input, moe_gain=moe_gain, expert_ids=expert_ids, route_weight=route_weight, gate_weight=gate_weight, up_weight=up_weight, down_weight=down_weight)


eps_norm = 1e-06

def reference(pool_input, pool_gain, mix_weight, moe_input, moe_gain, expert_ids, route_weight, gate_weight, up_weight, down_weight):
    values = pool_input.astype(jnp.float32)
    length = values.shape[0]
    running = jnp.concatenate([jnp.zeros((1, PW), jnp.float32), jnp.cumsum(values, axis=0)], axis=0)
    position = jnp.arange(length, dtype=jnp.int32)
    pieces = []
    for index_group in range(4):
        window = 2 ** (index_group + 1)
        begins = jnp.maximum(position + 1 - window, 0)
        counted = (position + 1 - begins).astype(jnp.float32)
        column = running[:, index_group * GROUP_CH:(index_group + 1) * GROUP_CH]
        pieces.append((column[1:] - column[begins]) / counted[:, None])
    pooled = ((jnp.concatenate(pieces, axis=1) - values) * pool_gain).astype(jnp.bfloat16)
    mixed_out = jnp.dot(pooled, mix_weight, preferred_element_type=jnp.float32).astype(jnp.bfloat16)
    inputs = moe_input.astype(jnp.float32)
    scale_rows = lax.rsqrt(lax.optimization_barrier(jnp.mean(inputs * inputs, axis=-1, keepdims=True)) + eps_norm)
    normed = (inputs * scale_rows * moe_gain).astype(jnp.bfloat16)
    blocks = TOK_B // ROWS_B
    chosen = expert_ids.reshape(blocks, ROWS_B * TOP)
    marked = (chosen[:, :, None] == jnp.arange(EXPERTS, dtype=jnp.int32)[None, None, :]).astype(jnp.int32)
    ranked = lax.optimization_barrier(jnp.sum((jnp.cumsum(marked, axis=1) - marked) * marked, axis=2)).astype(jnp.int32)
    owner_row = (jnp.arange(ROWS_B * TOP, dtype=jnp.int32)[None, :] // TOP + jnp.arange(blocks, dtype=jnp.int32)[:, None] * ROWS_B).astype(jnp.int32)
    block_ids = jnp.broadcast_to(jnp.arange(blocks, dtype=jnp.int32)[:, None], chosen.shape)
    source = jnp.full((EXPERTS, blocks, CAP), TOK_B, jnp.int32).at[chosen, block_ids, ranked].set(owner_row)
    padded = jnp.concatenate([normed, jnp.zeros((1, D), jnp.bfloat16)], axis=0)

    def expert_pass(operands):
        indices, gate_mat, up_mat, down_mat = operands
        gathered = padded[indices.reshape(-1)]
        gate_part = jnp.dot(gathered, gate_mat, preferred_element_type=jnp.float32)
        upward = jnp.dot(gathered, up_mat, preferred_element_type=jnp.float32)
        hidden = (jax.nn.silu(gate_part) * upward).astype(jnp.bfloat16)
        return jnp.dot(hidden, jnp.transpose(down_mat), preferred_element_type=jnp.float32).astype(jnp.bfloat16)
    results = lax.map(expert_pass, (source, gate_weight, up_weight, down_weight))
    flat_index = (chosen * (blocks * CAP) + block_ids * CAP + ranked).astype(jnp.int32)
    picked = results.reshape(EXPERTS * blocks * CAP, D)[flat_index.reshape(-1)].astype(jnp.float32)
    picked = picked.reshape(TOK_B, TOP, D)
    moe_out = lax.optimization_barrier(jnp.sum(picked * route_weight[:, :, None], axis=1)).astype(jnp.bfloat16)
    return (mixed_out, moe_out)
```

```python
import functools

import jax
import jax.numpy as jnp
from jax import lax
from jax.experimental import pallas as pl
from jax.experimental.pallas import tpu as pltpu
from jax.sharding import PartitionSpec as P

GROUP_CH = 256
EXPERTS = 16
CAP = 48
NX, NY, NZ = 4, 4, 8
EPS_NORM = 1e-06
DEV = pl.DeviceIdType.MESH

OFFSETS = (
    (0, 0), (1, 1), (3, 3), (0, 1), (0, 3), (2, 2), (1, 3), (3, 1),
    (1, 0), (3, 0), (2, 1), (2, 3), (1, 2), (3, 2), (0, 2), (2, 0),
)
SLOT_OF = {0: 0, 1: 1, -1: 2, 2: 3, -2: 4, 3: 5, -3: 6, 4: 7, -4: 7}
CW, CCW = 0, 1


def wait_for(ref, sem):
    pltpu.make_async_copy(ref, ref, sem).wait()


def kernel(
    gate_hbm, up_hbm, down_hbm, mix_hbm, pool_hbm, x_hbm,
    pool_gain, moe_gain, ids_ref, route_ref,
    mixed_hbm, moe_hbm,
    w_gate, w_up, w_down, w_mix,
    pool_in, halo, pooled, pooled_all, x_in, normed, placing, picking,
    outgoing, arrived, hidden, rows_out, rows_back, moe_vmem, mixed_vmem,
    load_sem, store_sem, ring_recv, ring_send, push_send, sib_gate, sib_up, sib_down, sib_mix,
    disp_send, disp_recv, halo_sem, pool_sem, ret_send, ret_recv,
):
    ep = lax.axis_index("ep")
    tp = lax.axis_index("tp")
    px, py = lax.rem(ep, NX), ep // NX
    pz, core = tp // 2, lax.rem(tp, 2)

    def plane(dx, dy):
        return (lax.rem(py + dy, NY) * NX + lax.rem(px + dx, NX), tp)

    def column(dz, dc):
        return (ep, lax.rem(pz + dz, NZ) * 2 + lax.rem(core + dc, 2))

    sibling = column(0, 1)
    ring_to = {CW: column(1, 0), CCW: column(NZ - 1, 0)}

    barrier = pltpu.get_barrier_semaphore()
    for dx, dy in OFFSETS[1:]:
        pl.semaphore_signal(barrier, inc=1, device_id=plane(dx, dy), device_id_type=DEV)
    for dz in range(NZ):
        for dc in range(2):
            if (dz, dc) != (0, 0):
                pl.semaphore_signal(barrier, inc=1, device_id=column(dz, dc), device_id_type=DEV)

    def piece(ref, index=None):
        def at(slot, other):
            rows = pl.ds(slot * 128 + 64 * other, 64)
            return ref.at[rows] if index is None else ref.at[index, rows]

        return at

    pieces = {"g": piece(w_gate), "u": piece(w_up)}
    hops = {"g": (4, 3), "u": (3, 4)}
    span = {"g": w_gate, "u": w_up}
    for q in range(4):
        pieces[f"d{q}"] = piece(w_down, q)
        hops[f"d{q}"] = (4, 3) if q % 2 == 0 else (3, 4)
        span[f"d{q}"] = w_down.at[q]
    for h in range(2):
        pieces[f"m{h}"] = piece(w_mix, h)
        hops[f"m{h}"] = (4, 3) if h == 0 else (3, 4)
        span[f"m{h}"] = w_mix.at[h]
    names = list(pieces)
    number = {name: k for k, name in enumerate(names)}

    loads = {}

    def load(name, src, dst):
        copy = pltpu.make_async_copy(src, dst, load_sem.at[len(loads)])
        copy.start()
        loads[name] = copy

    load("g", gate_hbm, w_gate.at[pl.ds(0, 64)])
    load("u", up_hbm, w_up.at[pl.ds(0, 64)])
    load("d0", down_hbm.at[:, pl.ds(0, 512)], w_down.at[0, pl.ds(0, 64)])
    load("x", x_hbm, x_in)
    load("pool", pool_hbm, pool_in)
    for q in range(1, 4):
        load(f"d{q}", down_hbm.at[:, pl.ds(512 * q, 512)], w_down.at[q, pl.ds(0, 64)])
    for h in range(2):
        load(f"m{h}", mix_hbm.at[:, pl.ds(1024 * h, 1024)], w_mix.at[h, pl.ds(0, 64)])

    def sib_sem(name, slot):
        if name == "g":
            return sib_gate.at[(0, 0, 0, 0, 1, 1, 2, 2)[slot]]
        if name == "u":
            return sib_up.at[(0, 0, 0, 0, 1, 1, 2, 2)[slot]]
        if name[0] == "d":
            return sib_down.at[int(name[1])]
        return sib_mix.at[int(name[1])]

    def ring_copy(name, way, hop):
        sign = -1 if way == CW else 1
        source, target = SLOT_OF[sign * (hop - 1)], SLOT_OF[sign * hop]
        at = pieces[name]
        return pltpu.make_async_remote_copy(
            src_ref=at(source, 0),
            dst_ref=at(target, 0),
            send_sem=ring_send.at[number[name]],
            recv_sem=ring_recv.at[number[name], way * 4 + hop - 1],
            device_id=ring_to[way],
            device_id_type=DEV,
        )

    def push(name, slot):
        at = pieces[name]
        pltpu.make_async_remote_copy(
            src_ref=at(slot, 0),
            dst_ref=at(slot, 1),
            send_sem=push_send.at[number[name]],
            recv_sem=sib_sem(name, slot),
            device_id=sibling,
            device_id_type=DEV,
        ).start()

    def first_sends(*pairs):
        for name, way in pairs:
            ring_copy(name, way, 1).start()

    def arrival(name, way, hop):
        if hop > hops[name][way]:
            return
        ring_copy(name, way, hop).wait_recv()
        if hop < hops[name][way]:
            ring_copy(name, way, hop + 1).start()
        push(name, SLOT_OF[-hop if way == CW else hop])

    def arrivals(hop, *pairs):
        for name, way in pairs:
            arrival(name, way, hop)

    set_one = (("g", CW), ("u", CCW), ("u", CW), ("g", CCW), ("d0", CW), ("d0", CCW))
    set_two = tuple((f"d{q}", way) for q in (1, 2, 3) for way in (CCW, CW))
    set_mix = (("m0", CW), ("m1", CCW), ("m1", CW), ("m0", CCW))

    pl.semaphore_wait(barrier, 30)

    loads["g"].wait()
    first_sends(("g", CW))
    loads["u"].wait()
    first_sends(*set_one[1:4])
    loads["d0"].wait()
    first_sends(*set_one[4:])

    loads["pool"].wait()
    halo_copy = pltpu.make_async_remote_copy(
        src_ref=pool_in.at[:, pl.ds(pool_in.shape[1] - 128, 128)],
        dst_ref=halo,
        send_sem=halo_sem.at[0],
        recv_sem=halo_sem.at[1],
        device_id=(lax.rem(ep + 1, EXPERTS), tp),
        device_id_type=DEV,
    )
    halo_copy.start()

    for name in ("g", "u", "d0"):
        push(name, 0)

    loads["x"].wait()
    gain_row = moe_gain[...]

    def norm_rows(k, carry):
        rows = pl.ds(k * 64, 64)
        v = x_in[rows, :].astype(jnp.float32)
        scale = lax.rsqrt(jnp.mean(v * v, axis=-1, keepdims=True) + EPS_NORM)
        normed[rows, :] = (v * scale * gain_row).astype(jnp.bfloat16)
        return carry

    lax.fori_loop(0, 4, norm_rows, 0)

    tokens = x_in.shape[0]
    expert = lax.broadcasted_iota(jnp.int32, (EXPERTS, tokens), 0)
    ids = ids_ref[...]
    chosen = [(ids[k : k + 1, :] == expert).astype(jnp.float32) for k in range(2)]
    marked = (chosen[0] + chosen[1]).astype(jnp.bfloat16)
    before = (
        lax.broadcasted_iota(jnp.int32, (tokens, tokens), 0)
        < lax.broadcasted_iota(jnp.int32, (tokens, tokens), 1)
    ).astype(jnp.bfloat16)
    rank = jnp.dot(marked, before, preferred_element_type=jnp.float32)
    away = lax.rem(expert // NX - py + NY, NY) * NX + lax.rem(lax.rem(expert, NX) - px + NX, NX)
    place = jnp.zeros((EXPERTS, tokens), jnp.float32)
    for p, (dx, dy) in enumerate(OFFSETS):
        place = jnp.where(away == dy * NX + dx, float(p * CAP), place)
    slot_of = place + rank
    slots = [
        jnp.sum(chosen[k] * slot_of, axis=0, keepdims=True).astype(jnp.int32) for k in range(2)
    ]

    def disp_copy(p):
        dx, dy = OFFSETS[p]
        rows = pl.ds(p * CAP, CAP)
        return pltpu.make_async_remote_copy(
            src_ref=outgoing.at[rows],
            dst_ref=arrived.at[rows],
            send_sem=disp_send,
            recv_sem=disp_recv.at[0 if p < 8 else 1],
            device_id=plane(dx, dy),
            device_id_type=DEV,
        )

    for group in range(4):
        row_ids = lax.broadcasted_iota(jnp.int32, (4 * CAP, tokens), 0) + group * 4 * CAP
        hit = (row_ids == slots[0]) | (row_ids == slots[1])
        placing[...] = hit.astype(jnp.bfloat16)

        def place_columns(n, carry, group=group):
            cols = pl.ds(pl.multiple_of(n * 512, 512), 512)
            block = jnp.dot(
                placing[...], normed[:, cols], preferred_element_type=jnp.float32
            ).astype(jnp.bfloat16)
            outgoing[pl.ds(group * 4 * CAP, 4 * CAP), cols] = block
            if group == 0:
                arrived[pl.ds(0, CAP), cols] = block[:CAP]
            return carry

        lax.fori_loop(0, 4, place_columns, 0)
        for p in range(max(1, group * 4), group * 4 + 4):
            disp_copy(p).start()

    arrivals(1, *set_one)

    route = route_ref[...]
    slot_rows = lax.broadcasted_iota(jnp.int32, (EXPERTS * CAP, tokens), 0)
    weighted = jnp.where(slot_rows == slots[0], route[0:1, :], 0.0) + jnp.where(
        slot_rows == slots[1], route[1:2, :], 0.0
    )
    picking[...] = weighted.T.astype(jnp.bfloat16)

    halo_copy.wait_recv()
    row_count = pool_in.shape[1]
    window_group = (tp * 64) // GROUP_CH
    gain_wide = pool_gain[...]
    diagonal = lax.broadcasted_iota(jnp.int32, (64, 64), 0) == lax.broadcasted_iota(
        jnp.int32, (64, 64), 1
    )
    gain_col = jnp.sum(jnp.where(diagonal, gain_wide, 0.0), axis=1, keepdims=True)
    for part in range(4):
        r = slice(part * 16, part * 16 + 16)
        values = pool_in[r, :].astype(jnp.float32)
        carried = jnp.where(ep > 0, halo[r, :].astype(jnp.float32), 0.0)
        level = jnp.concatenate([carried, values], axis=1)
        summed = jnp.zeros_like(values)
        for doubling in range(4):
            level = level + pltpu.roll(level, 2**doubling, 1)
            summed = jnp.where(window_group == doubling, level[:, 128:], summed)
        position = ep * row_count + lax.broadcasted_iota(jnp.int32, (1, row_count), 1)
        width = 2 ** 1
        for doubling in range(1, 4):
            width = jnp.where(window_group == doubling, 2 ** (doubling + 1), width)
        counted = jnp.minimum(position + 1, width).astype(jnp.float32)
        pooled[r, :] = ((summed / counted - values) * gain_col[r, :]).astype(jnp.bfloat16)
    pooled_all[pl.ds(0, 64), :] = pooled[:, pl.ds(pl.multiple_of(tp * 128, 128), 128)]

    def pool_copy(dz, dc):
        target = lax.rem(pz + dz, NZ) * 2 + lax.rem(core + dc, 2)
        rel = -dz if dz <= 4 else NZ - dz
        return pltpu.make_async_remote_copy(
            src_ref=pooled.at[:, pl.ds(pl.multiple_of(target * 128, 128), 128)],
            dst_ref=pooled_all.at[pl.ds(SLOT_OF[rel] * 128 + 64 * dc, 64)],
            send_sem=pool_sem.at[0],
            recv_sem=pool_sem.at[1],
            device_id=column(dz, dc),
            device_id_type=DEV,
        )

    half_rows = 8 * CAP

    def expert_chunk(half, chunk):
        rows = pl.ds(pl.multiple_of(half * half_rows, half_rows), half_rows)
        cols = pl.ds(pl.multiple_of(chunk * 256, 256), 256)
        r = arrived[rows, :]
        dims = (((1,), (1,)), ((), ()))
        gate_part = lax.dot_general(r, w_gate[cols, :], dims, preferred_element_type=jnp.float32)
        upward = lax.dot_general(r, w_up[cols, :], dims, preferred_element_type=jnp.float32)
        act = gate_part / (1.0 + jnp.exp(-gate_part)) * upward
        hidden[rows, cols] = act.astype(jnp.bfloat16)

    def expert_chunks(half, begin, end):
        def one(chunk, carry):
            expert_chunk(half, chunk)
            return carry

        lax.fori_loop(begin, end, one, 0)

    def ret_copy(q, p):
        dx, dy = OFFSETS[p]
        rows = pl.ds(p * CAP, CAP)
        return pltpu.make_async_remote_copy(
            src_ref=rows_out.at[q, rows],
            dst_ref=rows_back.at[q, rows],
            send_sem=ret_send.at[q],
            recv_sem=ret_recv.at[q],
            device_id=plane(NX - dx, NY - dy),
            device_id_type=DEV,
        )

    def give_back(q):
        wait_for(w_down.at[q, pl.ds(0, 512)], sib_down.at[q])
        for half in range(2):
            rows = pl.ds(half * half_rows, half_rows)
            block = jnp.dot(
                hidden[rows, :], w_down[q], preferred_element_type=jnp.float32
            ).astype(jnp.bfloat16)
            rows_out[q, rows] = block
            if half == 0:
                rows_back[q, pl.ds(0, CAP)] = block[:CAP]
            for p in range(max(1, half * 8), half * 8 + 8):
                ret_copy(q, p).start()

    def moe_store(q):
        cols = pl.ds(q * 512, 512)
        return pltpu.make_async_copy(moe_vmem.at[q], moe_hbm.at[:, cols], store_sem.at[q])

    def combine(q):
        wait_for(rows_back.at[q, pl.ds(CAP, 15 * CAP)], ret_recv.at[q])
        moe_vmem[q] = jnp.dot(
            picking[...], rows_back[q], preferred_element_type=jnp.float32
        ).astype(jnp.bfloat16)
        moe_store(q).start()

    arrivals(2, *set_one)

    wait_for(arrived.at[pl.ds(CAP, 7 * CAP)], disp_recv.at[0])
    wait_for(w_gate.at[pl.ds(0, 256)], sib_gate.at[0])
    wait_for(w_up.at[pl.ds(0, 256)], sib_up.at[0])
    expert_chunks(0, 0, 2)

    arrivals(3, *set_one)
    for q in range(1, 4):
        loads[f"d{q}"].wait()
    first_sends(*set_two)
    for q in range(1, 4):
        push(f"d{q}", 0)
    wait_for(w_gate.at[pl.ds(0, 128)], sib_gate.at[1])
    wait_for(w_up.at[pl.ds(0, 128)], sib_up.at[1])
    expert_chunks(0, 2, 3)
    wait_for(arrived.at[pl.ds(8 * CAP, 8 * CAP)], disp_recv.at[1])
    expert_chunks(1, 0, 3)
    arrivals(4, *set_one)
    arrivals(1, *set_two)
    wait_for(w_gate.at[pl.ds(0, 128)], sib_gate.at[2])
    wait_for(w_up.at[pl.ds(0, 128)], sib_up.at[2])
    expert_chunks(0, 3, 4)
    expert_chunks(1, 3, 4)
    give_back(0)
    arrivals(2, *set_two)
    arrivals(3, *set_two)
    for dz in (4, 3, 5, 2, 6, 1, 7, 0):
        for dc in range(2):
            if (dz, dc) != (0, 0):
                pool_copy(dz, dc).start()
    for h in range(2):
        loads[f"m{h}"].wait()
    first_sends(*set_mix)
    for h in range(2):
        push(f"m{h}", 0)
    arrivals(4, *set_two)
    give_back(1)
    give_back(2)
    give_back(3)
    arrivals(1, *set_mix)
    combine(0)
    arrivals(2, *set_mix)
    combine(1)
    arrivals(3, *set_mix)
    combine(2)
    arrivals(4, *set_mix)

    wait_for(pooled_all.at[pl.ds(64, 960)], pool_sem.at[1])
    pooled_rows = pooled_all[...].astype(jnp.float32).T.astype(jnp.bfloat16)
    for h in range(2):
        wait_for(w_mix.at[h, pl.ds(0, 512)], sib_mix.at[h])
        mixed_vmem[h] = jnp.dot(
            pooled_rows, w_mix[h], preferred_element_type=jnp.float32
        ).astype(jnp.bfloat16)
        pltpu.make_async_copy(
            mixed_vmem.at[h], mixed_hbm.at[:, pl.ds(h * 1024, 1024)], store_sem.at[4 + h]
        ).start()
    combine(3)

    for name in names:
        whole = span[name]
        wait_for(whole.at[pl.ds(0, 7 * 64)], ring_send.at[number[name]])
        wait_for(whole.at[pl.ds(0, 8 * 64)], push_send.at[number[name]])
    wait_for(outgoing.at[pl.ds(CAP, 15 * CAP)], disp_send)
    halo_copy.wait_send()
    wait_for(pooled_all.at[pl.ds(64, 960)], pool_sem.at[0])
    for q in range(4):
        wait_for(rows_out.at[q, pl.ds(CAP, 15 * CAP)], ret_send.at[q])
        moe_store(q).wait()
    for h in range(2):
        pltpu.make_async_copy(
            mixed_vmem.at[h], mixed_hbm.at[:, pl.ds(h * 1024, 1024)], store_sem.at[4 + h]
        ).wait()


def body(
    pool_input,
    pool_gain,
    mix_weight,
    moe_input,
    moe_gain,
    expert_ids,
    route_weight,
    gate_weight,
    up_weight,
    down_weight,
):
    rows_a, channels = pool_input.shape
    tokens, width = moe_input.shape
    slots = EXPERTS * CAP
    bf, f32 = jnp.bfloat16, jnp.float32
    hbm = pl.BlockSpec(memory_space=pl.ANY)
    vmem = pl.BlockSpec(memory_space=pltpu.VMEM)
    dma = pltpu.SemaphoreType.DMA
    return pl.pallas_call(
        kernel,
        out_shape=(
            jax.ShapeDtypeStruct((rows_a // 16, width), bf),
            jax.ShapeDtypeStruct((tokens, width), bf),
        ),
        in_specs=[hbm] * 6 + [vmem] * 4,
        out_specs=(hbm, hbm),
        scratch_shapes=[
            pltpu.VMEM((1024, width), bf),
            pltpu.VMEM((1024, width), bf),
            pltpu.VMEM((4, 1024, 512), bf),
            pltpu.VMEM((2, 1024, 1024), bf),
            pltpu.VMEM((channels, rows_a), bf),
            pltpu.VMEM((channels, 128), bf),
            pltpu.VMEM((channels, rows_a), bf),
            pltpu.VMEM((1024, 128), bf),
            pltpu.VMEM((tokens, width), bf),
            pltpu.VMEM((tokens, width), bf),
            pltpu.VMEM((4 * CAP, tokens), bf),
            pltpu.VMEM((tokens, slots), bf),
            pltpu.VMEM((slots, width), bf),
            pltpu.VMEM((slots, width), bf),
            pltpu.VMEM((slots, 1024), bf),
            pltpu.VMEM((4, slots, 512), bf),
            pltpu.VMEM((4, slots, 512), bf),
            pltpu.VMEM((4, tokens, 512), bf),
            pltpu.VMEM((2, rows_a // 16, 1024), bf),
            dma((10,)),
            dma((6,)),
            dma((8, 8)),
            dma((8,)),
            dma((8,)),
            dma((3,)),
            dma((3,)),
            dma((4,)),
            dma((2,)),
            dma,
            dma((2,)),
            dma((2,)),
            dma((2,)),
            dma((4,)),
            dma((4,)),
        ],
        compiler_params=pltpu.CompilerParams(
            collective_id=0, has_side_effects=True, vmem_limit_bytes=60 << 20
        ),
        name="mixer_and_experts",
    )(
        gate_weight[0].T,
        up_weight[0].T,
        down_weight[0].T,
        mix_weight,
        pool_input.T,
        moe_input,
        pool_gain.reshape(1, channels),
        moe_gain.reshape(1, width),
        expert_ids.T,
        route_weight.T,
    )


def solution(mesh):
    return jax.shard_map(
        body,
        mesh=mesh,
        in_specs=(
            P("ep", "tp"),
            P("tp"),
            P("tp", None),
            P(("ep", "tp"), None),
            P(),
            P(("ep", "tp"), None),
            P(("ep", "tp"), None),
            P("ep", None, "tp"),
            P("ep", None, "tp"),
            P("ep", None, "tp"),
        ),
        out_specs=(P(("ep", "tp"), None), P(("ep", "tp"), None)),
        check_vma=False,
    )
```

```python
import functools

import jax
import jax.numpy as jnp
from jax import lax
from jax.experimental import pallas as pl
from jax.experimental.pallas import tpu as pltpu
from jax.sharding import PartitionSpec as P

GROUP_CH = 256
EXPERTS = 16
CAP = 48
NX, NY, NZ = 4, 4, 8
EPS_NORM = 1e-06
DEV = pl.DeviceIdType.MESH

OFFSETS = (
    (0, 0), (1, 1), (3, 3), (0, 1), (0, 3), (2, 2), (1, 3), (3, 1),
    (1, 0), (3, 0), (2, 1), (2, 3), (1, 2), (3, 2), (0, 2), (2, 0),
)
SLOT_OF = {0: 0, 1: 1, -1: 2, 2: 3, -2: 4, 3: 5, -3: 6, 4: 7, -4: 7}
CW, CCW = 0, 1


phase = jax.named_scope


def wait_for(ref, sem):
    pltpu.make_async_copy(ref, ref, sem).wait()


def kernel(
    gate_hbm, up_hbm, down_hbm, mix_hbm, pool_hbm, x_hbm,
    pool_gain, moe_gain, ids_ref, route_ref,
    mixed_ref, moe_ref,
    w_in, w_down, w_mix,
    pool_in, halo, pooled, pooled_all, x_in, normed, placing, picking,
    outgoing, arrived, hidden, rows_out, rows_back, pooled_rows, mixed_sum,
    load_sem, ring_recv, ring_send, push_send, sib_in, sib_down, sib_mix,
    disp_send, disp_recv, halo_sem, pool_sem, ret_send, ret_recv,
):
    ep = lax.axis_index("ep")
    tp = lax.axis_index("tp")
    px, py = lax.rem(ep, NX), ep // NX
    pz, core = tp // 2, lax.rem(tp, 2)

    def plane(dx, dy):
        return (lax.rem(py + dy, NY) * NX + lax.rem(px + dx, NX), tp)

    def column(dz, dc):
        return (ep, lax.rem(pz + dz, NZ) * 2 + lax.rem(core + dc, 2))

    sibling = column(0, 1)
    ring_to = {CW: column(1, 0), CCW: column(NZ - 1, 0)}

    barrier = pltpu.get_barrier_semaphore()
    for dx, dy in OFFSETS[1:]:
        pl.semaphore_signal(barrier, inc=1, device_id=plane(dx, dy), device_id_type=DEV)
    for dz in range(NZ):
        for dc in range(2):
            if (dz, dc) != (0, 0):
                pl.semaphore_signal(barrier, inc=1, device_id=column(dz, dc), device_id_type=DEV)

    def piece(ref, index=None):
        def at(slot, other):
            rows = pl.ds(slot * 128 + 64 * other, 64)
            return ref.at[rows] if index is None else ref.at[index, rows]

        return at

    pieces = {
        "g": lambda slot, other: w_in.at[slot, pl.ds(64 * other, 64)],
        "u": lambda slot, other: w_in.at[slot, pl.ds(128 + 64 * other, 64)],
    }
    hops = {"g": (4, 3), "u": (3, 4)}
    for q in range(4):
        pieces[f"d{q}"] = piece(w_down, q)
        hops[f"d{q}"] = (4, 3) if q % 2 == 0 else (3, 4)
    for h in range(2):
        pieces[f"m{h}"] = piece(w_mix, h)
        hops[f"m{h}"] = (4, 3) if h == 0 else (3, 4)
    names = list(pieces)
    number = {name: k for k, name in enumerate(names)}

    loads = {}

    def load(name, src, dst):
        copy = pltpu.make_async_copy(src, dst, load_sem.at[len(loads)])
        copy.start()
        loads[name] = copy

    load("g", gate_hbm, w_in.at[0, pl.ds(0, 64)])
    load("u", up_hbm, w_in.at[0, pl.ds(128, 64)])
    load("d0", down_hbm.at[:, pl.ds(0, 512)], w_down.at[0, pl.ds(0, 64)])
    load("x", x_hbm, x_in)
    load("pool", pool_hbm, pool_in)
    for q in range(1, 4):
        load(f"d{q}", down_hbm.at[:, pl.ds(512 * q, 512)], w_down.at[q, pl.ds(0, 64)])
    for h in range(2):
        load(f"m{h}", mix_hbm.at[:, pl.ds(1024 * h, 1024)], w_mix.at[h, pl.ds(0, 64)])

    def sib_sem(name, slot):
        if name in "gu":
            return sib_in.at[number[name], (0, 0, 0, 1, 1, 2, 2, 3)[slot]]
        if name[0] == "d":
            return sib_down.at[int(name[1])]
        return sib_mix.at[int(name[1]), slot // 7]

    def ring_copy(name, way, hop):
        sign = -1 if way == CW else 1
        source, target = SLOT_OF[sign * (hop - 1)], SLOT_OF[sign * hop]
        at = pieces[name]
        return pltpu.make_async_remote_copy(
            src_ref=at(source, 0),
            dst_ref=at(target, 0),
            send_sem=ring_send.at[number[name]],
            recv_sem=ring_recv.at[number[name], way * 4 + hop - 1],
            device_id=ring_to[way],
            device_id_type=DEV,
        )

    def push(name, slot):
        at = pieces[name]
        pltpu.make_async_remote_copy(
            src_ref=at(slot, 0),
            dst_ref=at(slot, 1),
            send_sem=push_send.at[number[name]],
            recv_sem=sib_sem(name, slot),
            device_id=sibling,
            device_id_type=DEV,
        ).start()

    def first_sends(*pairs):
        for name, way in pairs:
            ring_copy(name, way, 1).start()

    def arrival(name, way, hop):
        if hop > hops[name][way]:
            return
        ring_copy(name, way, hop).wait_recv()
        if hop < hops[name][way]:
            ring_copy(name, way, hop + 1).start()
        push(name, SLOT_OF[-hop if way == CW else hop])

    def arrivals(hop, *pairs):
        for name, way in pairs:
            arrival(name, way, hop)

    set_one = (("g", CW), ("u", CCW), ("u", CW), ("g", CCW), ("d0", CW), ("d0", CCW))
    set_mix = (("m0", CW), ("m1", CCW), ("m1", CW), ("m0", CCW))

    def both(name):
        return ((name, CCW), (name, CW))

    with phase("enter"):
        pl.semaphore_wait(barrier, 30)
    with phase("first"):
        loads["g"].wait()
        first_sends(("g", CW))
        loads["u"].wait()
        first_sends(*set_one[1:4])
        loads["d0"].wait()
        first_sends(*set_one[4:])

    loads["pool"].wait()
    halo_copy = pltpu.make_async_remote_copy(
        src_ref=pool_in.at[:, pl.ds(pool_in.shape[1] - 128, 128)],
        dst_ref=halo,
        send_sem=halo_sem.at[0],
        recv_sem=halo_sem.at[1],
        device_id=(lax.rem(ep + 1, EXPERTS), tp),
        device_id_type=DEV,
    )
    halo_copy.start()

    for name in ("g", "u", "d0"):
        push(name, 0)

    loads["x"].wait()
    gain_row = moe_gain[...]

    def norm_rows(k, carry):
        rows = pl.ds(k * 64, 64)
        v = x_in[rows, :].astype(jnp.float32)
        scale = lax.rsqrt(jnp.mean(v * v, axis=-1, keepdims=True) + EPS_NORM)
        normed[rows, :] = (v * scale * gain_row).astype(jnp.bfloat16)
        return carry

    with phase("norm"):
        lax.fori_loop(0, 4, norm_rows, 0)

    tokens = x_in.shape[0]
    expert = lax.broadcasted_iota(jnp.int32, (EXPERTS, tokens), 0)
    ids = ids_ref[...]
    chosen = [(ids[k : k + 1, :] == expert).astype(jnp.float32) for k in range(2)]
    marked = (chosen[0] + chosen[1]).astype(jnp.bfloat16)
    before = (
        lax.broadcasted_iota(jnp.int32, (tokens, tokens), 0)
        < lax.broadcasted_iota(jnp.int32, (tokens, tokens), 1)
    ).astype(jnp.bfloat16)
    rank = jnp.dot(marked, before, preferred_element_type=jnp.float32)
    away = lax.rem(expert // NX - py + NY, NY) * NX + lax.rem(lax.rem(expert, NX) - px + NX, NX)
    place = jnp.zeros((EXPERTS, tokens), jnp.float32)
    for p, (dx, dy) in enumerate(OFFSETS):
        place = jnp.where(away == dy * NX + dx, float(p * CAP), place)
    slot_of = place + rank
    slots = [
        jnp.sum(chosen[k] * slot_of, axis=0, keepdims=True).astype(jnp.int32) for k in range(2)
    ]

    def disp_copy(p):
        dx, dy = OFFSETS[p]
        rows = pl.ds(p * CAP, CAP)
        return pltpu.make_async_remote_copy(
            src_ref=outgoing.at[rows],
            dst_ref=arrived.at[rows],
            send_sem=disp_send,
            recv_sem=disp_recv.at[p // 8],
            device_id=plane(dx, dy),
            device_id_type=DEV,
        )

    for group in range(4):
        row_ids = lax.broadcasted_iota(jnp.int32, (4 * CAP, tokens), 0) + group * 4 * CAP
        hit = (row_ids == slots[0]) | (row_ids == slots[1])
        placing[...] = hit.astype(jnp.bfloat16)

        def place_columns(n, carry, group=group):
            cols = pl.ds(pl.multiple_of(n * 512, 512), 512)
            block = jnp.dot(
                placing[...], normed[:, cols], preferred_element_type=jnp.float32
            ).astype(jnp.bfloat16)
            outgoing[pl.ds(group * 4 * CAP, 4 * CAP), cols] = block
            if group == 0:
                arrived[pl.ds(0, CAP), cols] = block[:CAP]
            return carry

        lax.fori_loop(0, 4, place_columns, 0)
        if group < 2:
            for p in range(max(1, group * 4), group * 4 + 4):
                disp_copy(p).start()

    with phase("one_1"):
        arrivals(1, *set_one)
    for p in range(8, 16):
        disp_copy(p).start()
    loads["d1"].wait()
    first_sends(*both("d1"))
    push("d1", 0)

    route = route_ref[...]
    slot_rows = lax.broadcasted_iota(jnp.int32, (EXPERTS * CAP, tokens), 0)
    weighted = jnp.where(slot_rows == slots[0], route[0:1, :], 0.0) + jnp.where(
        slot_rows == slots[1], route[1:2, :], 0.0
    )
    picking[...] = weighted.T.astype(jnp.bfloat16)

    with phase("halo"):
        halo_copy.wait_recv()
    row_count = pool_in.shape[1]
    window_group = (tp * 64) // GROUP_CH
    gain_wide = pool_gain[...]
    diagonal = lax.broadcasted_iota(jnp.int32, (64, 64), 0) == lax.broadcasted_iota(
        jnp.int32, (64, 64), 1
    )
    gain_col = jnp.sum(jnp.where(diagonal, gain_wide, 0.0), axis=1, keepdims=True)
    for part in range(4):
        r = slice(part * 16, part * 16 + 16)
        values = pool_in[r, :].astype(jnp.float32)
        carried = jnp.where(ep > 0, halo[r, :].astype(jnp.float32), 0.0)
        level = jnp.concatenate([carried, values], axis=1)
        summed = jnp.zeros_like(values)
        for doubling in range(4):
            level = level + pltpu.roll(level, 2**doubling, 1)
            summed = jnp.where(window_group == doubling, level[:, 128:], summed)
        position = ep * row_count + lax.broadcasted_iota(jnp.int32, (1, row_count), 1)
        width = 2 ** 1
        for doubling in range(1, 4):
            width = jnp.where(window_group == doubling, 2 ** (doubling + 1), width)
        counted = jnp.minimum(position + 1, width).astype(jnp.float32)
        pooled[r, :] = ((summed / counted - values) * gain_col[r, :]).astype(jnp.bfloat16)
    pooled_all[pl.ds(0, 64), :] = pooled[:, pl.ds(pl.multiple_of(tp * 128, 128), 128)]

    def pool_copy(dz, dc):
        target = lax.rem(pz + dz, NZ) * 2 + lax.rem(core + dc, 2)
        rel = -dz if dz <= 4 else NZ - dz
        return pltpu.make_async_remote_copy(
            src_ref=pooled.at[:, pl.ds(pl.multiple_of(target * 128, 128), 128)],
            dst_ref=pooled_all.at[pl.ds(SLOT_OF[rel] * 128 + 64 * dc, 64)],
            send_sem=pool_sem.at[0],
            recv_sem=pool_sem.at[1],
            device_id=column(dz, dc),
            device_id_type=DEV,
        )

    half_rows = 8 * CAP

    def gated(both_parts):
        gate_part, upward = both_parts[:, :128], both_parts[:, 128:]
        return (gate_part / (1.0 + jnp.exp(-gate_part)) * upward).astype(jnp.bfloat16)

    def project(rows, weights):
        return lax.dot_general(
            arrived[rows, :], weights, (((1,), (1,)), ((), ())), preferred_element_type=jnp.float32
        )

    def hidden_pairs(half, first_slot, pairs):
        rows = pl.ds(half * half_rows, half_rows)

        def one(pair, carry):
            slot = first_slot + 2 * pair
            sums = project(rows, w_in[pl.ds(slot, 2)].reshape(512, w_in.shape[2]))
            for k in range(2):
                cols = pl.ds(pl.multiple_of((slot + k) * 128, 128), 128)
                hidden[rows, cols] = gated(sums[:, 256 * k : 256 * k + 256])
            return carry

        lax.fori_loop(0, pairs, one, 0)

    def ret_copy(q, p):
        dx, dy = OFFSETS[p]
        rows = pl.ds(p * CAP, CAP)
        return pltpu.make_async_remote_copy(
            src_ref=rows_out.at[q, rows],
            dst_ref=rows_back.at[q, rows],
            send_sem=ret_send.at[q],
            recv_sem=ret_recv.at[q],
            device_id=plane(NX - dx, NY - dy),
            device_id_type=DEV,
        )

    def give_back(q, half):
        rows = pl.ds(half * half_rows, half_rows)
        block = jnp.dot(
            hidden[rows, :], w_down[q], preferred_element_type=jnp.float32
        ).astype(jnp.bfloat16)
        rows_out[q, rows] = block
        if half == 0:
            rows_back[q, pl.ds(0, CAP)] = block[:CAP]
        for p in range(max(1, half * 8), half * 8 + 8):
            ret_copy(q, p).start()

    def combine(q):
        wait_for(rows_back.at[q, pl.ds(CAP, 15 * CAP)], ret_recv.at[q])
        moe_ref[:, pl.ds(q * 512, 512)] = jnp.dot(
            picking[...], rows_back[q], preferred_element_type=jnp.float32
        ).astype(jnp.bfloat16)

    def down_ready(q):
        wait_for(w_down.at[q, pl.ds(0, 512)], sib_down.at[q])

    def in_ready(hop):
        for part in range(2):
            if hop == 1:
                wait_for(arrived.at[pl.ds(0, 192)], sib_in.at[part, 0])
            else:
                wait_for(w_in.at[0, pl.ds(0, 64 if hop == 4 else 128)], sib_in.at[part, hop - 1])

    with phase("in_1"):
        in_ready(1)
    with phase("one_2"):
        arrivals(2, *set_one)
    with phase("d1_1"):
        arrivals(1, *both("d1"))
    with phase("disp_0"):
        wait_for(arrived.at[pl.ds(CAP, 7 * CAP)], disp_recv.at[0])
        in_ready(2)
    with phase("hid_a"):
        hidden_pairs(0, 0, 2)
    with phase("one_3"):
        arrivals(3, *set_one)
    with phase("d1_2"):
        arrivals(2, *both("d1"))
    for q in (2, 3):
        loads[f"d{q}"].wait()
        first_sends(*both(f"d{q}"))
        push(f"d{q}", 0)
    with phase("in_3"):
        in_ready(3)
    with phase("hid_b"):
        hidden_pairs(0, 4, 1)
    with phase("disp_1"):
        wait_for(arrived.at[pl.ds(8 * CAP, 8 * CAP)], disp_recv.at[1])
    with phase("hid_c"):
        hidden_pairs(1, 0, 3)
    with phase("one_4"):
        arrivals(4, *set_one[:4])
    with phase("one_4d"):
        arrivals(4, *set_one[4:])
    with phase("in_4"):
        in_ready(4)
    with phase("hid_67a"):
        hidden_pairs(0, 6, 1)
    with phase("d0"):
        down_ready(0)
    with phase("give_0a"):
        give_back(0, 0)
    with phase("hid_67b"):
        hidden_pairs(1, 6, 1)
    with phase("give_0b"):
        give_back(0, 1)
    with phase("two_1"):
        arrivals(3, *both("d1"))
        arrivals(1, *both("d2"))
        arrivals(1, *both("d3"))
    with phase("two_2"):
        arrivals(4, *both("d1"))
        arrivals(2, *both("d2"))
        arrivals(2, *both("d3"))
    for h in range(2):
        loads[f"m{h}"].wait()
    first_sends(*set_mix[:2])
    with phase("d1"):
        down_ready(1)
    with phase("give_1"):
        give_back(1, 0)
        give_back(1, 1)
    with phase("two_3"):
        arrivals(3, *both("d2"))
        arrivals(3, *both("d3"))
    first_sends(*set_mix[2:])
    for h in range(2):
        push(f"m{h}", 0)
    for dz in (4, 3, 5, 2, 6, 1, 7, 0):
        for dc in range(2):
            if (dz, dc) != (0, 0):
                pool_copy(dz, dc).start()
    with phase("mix_1a"):
        arrivals(1, *set_mix[:2])
    with phase("two_4"):
        arrivals(4, *both("d2"))
        arrivals(4, *both("d3"))
    with phase("d2"):
        down_ready(2)
    with phase("give_2"):
        give_back(2, 0)
        give_back(2, 1)
    with phase("d3"):
        down_ready(3)
    with phase("give_3"):
        give_back(3, 0)
        give_back(3, 1)
    with phase("mix_1b"):
        arrivals(1, *set_mix[2:])
    with phase("combine_0"):
        combine(0)
    with phase("mix_2"):
        arrivals(2, *set_mix)
    with phase("combine_1"):
        combine(1)
    with phase("pool_wait"):
        wait_for(pooled_all.at[pl.ds(64, 960)], pool_sem.at[1])
    pooled_rows[...] = pooled_all[...].astype(jnp.float32).T.astype(jnp.bfloat16)
    with phase("mix_3"):
        arrivals(3, *set_mix)

    for h in range(2):
        wait_for(w_mix.at[h, pl.ds(0, 448)], sib_mix.at[h, 0])
    with phase("mixer"):
        for h in range(2):
            mixed_sum[h] = jnp.dot(
                pooled_rows[:, :896], w_mix[h, :896], preferred_element_type=jnp.float32
            )
    with phase("combine_2"):
        combine(2)
    with phase("mix_4"):
        arrivals(4, *set_mix)
        for h in range(2):
            wait_for(w_mix.at[h, pl.ds(0, 64)], sib_mix.at[h, 1])
    with phase("mixer_2"):
        for h in range(2):
            last = jnp.dot(pooled_rows[:, 896:], w_mix[h, 896:], preferred_element_type=jnp.float32)
            mixed_ref[:, pl.ds(h * 1024, 1024)] = (mixed_sum[h] + last).astype(jnp.bfloat16)
    with phase("combine_3"):
        combine(3)

    for name in names:
        if name in "gu":
            sent, pushed = outgoing.at[pl.ds(0, 7 * 64)], outgoing.at[pl.ds(0, 8 * 64)]
        else:
            whole = w_down.at[int(name[1])] if name[0] == "d" else w_mix.at[int(name[1])]
            sent, pushed = whole.at[pl.ds(0, 7 * 64)], whole.at[pl.ds(0, 8 * 64)]
        wait_for(sent, ring_send.at[number[name]])
        wait_for(pushed, push_send.at[number[name]])
    wait_for(outgoing.at[pl.ds(CAP, 15 * CAP)], disp_send)
    halo_copy.wait_send()
    wait_for(pooled_all.at[pl.ds(64, 960)], pool_sem.at[0])
    for q in range(4):
        wait_for(rows_out.at[q, pl.ds(CAP, 15 * CAP)], ret_send.at[q])


def body(
    pool_input,
    pool_gain,
    mix_weight,
    moe_input,
    moe_gain,
    expert_ids,
    route_weight,
    gate_weight,
    up_weight,
    down_weight,
):
    rows_a, channels = pool_input.shape
    tokens, width = moe_input.shape
    slots = EXPERTS * CAP
    bf, f32 = jnp.bfloat16, jnp.float32
    hbm = pl.BlockSpec(memory_space=pl.ANY)
    vmem = pl.BlockSpec(memory_space=pltpu.VMEM)
    dma = pltpu.SemaphoreType.DMA
    return pl.pallas_call(
        kernel,
        out_shape=(
            pltpu.VMEM((rows_a // 16, width), bf),
            pltpu.VMEM((tokens, width), bf),
        ),
        in_specs=[hbm] * 6 + [vmem] * 4,
        out_specs=(vmem, vmem),
        scratch_shapes=[
            pltpu.VMEM((8, 256, width), bf),
            pltpu.VMEM((4, 1024, 512), bf),
            pltpu.VMEM((2, 1024, 1024), bf),
            pltpu.VMEM((channels, rows_a), bf),
            pltpu.VMEM((channels, 128), bf),
            pltpu.VMEM((channels, rows_a), bf),
            pltpu.VMEM((1024, 128), bf),
            pltpu.VMEM((tokens, width), bf),
            pltpu.VMEM((tokens, width), bf),
            pltpu.VMEM((4 * CAP, tokens), bf),
            pltpu.VMEM((tokens, slots), bf),
            pltpu.VMEM((slots, width), bf),
            pltpu.VMEM((slots, width), bf),
            pltpu.VMEM((slots, 1024), bf),
            pltpu.VMEM((4, slots, 512), bf),
            pltpu.VMEM((4, slots, 512), bf),
            pltpu.VMEM((rows_a // 16, 1024), bf),
            pltpu.VMEM((2, rows_a // 16, 1024), f32),
            dma((10,)),
            dma((8, 8)),
            dma((8,)),
            dma((8,)),
            dma((2, 4)),
            dma((4,)),
            dma((2, 2)),
            dma,
            dma((2,)),
            dma((2,)),
            dma((2,)),
            dma((4,)),
            dma((4,)),
        ],
        compiler_params=pltpu.CompilerParams(
            collective_id=0, has_side_effects=True, vmem_limit_bytes=56 << 20
        ),
        name="mixer_and_experts",
    )(
        gate_weight[0].T,
        up_weight[0].T,
        down_weight[0].T,
        mix_weight,
        pool_input.T,
        moe_input,
        pool_gain.reshape(1, channels),
        moe_gain.reshape(1, width),
        expert_ids.T,
        route_weight.T,
    )


def solution(mesh):
    return jax.shard_map(
        body,
        mesh=mesh,
        in_specs=(
            P("ep", "tp"),
            P("tp"),
            P("tp", None),
            P(("ep", "tp"), None),
            P(),
            P(("ep", "tp"), None),
            P(("ep", "tp"), None),
            P("ep", None, "tp"),
            P("ep", None, "tp"),
            P("ep", None, "tp"),
        ),
        out_specs=(P(("ep", "tp"), None), P(("ep", "tp"), None)),
        check_vma=False,
    )
```

```python
import functools

import jax
import jax.numpy as jnp
from jax import lax
from jax.experimental import pallas as pl
from jax.experimental.pallas import tpu as pltpu
from jax.sharding import PartitionSpec as P

GROUP_CH = 256
EXPERTS = 16
CAP = 48
NX, NY, NZ = 4, 4, 8
EPS_NORM = 1e-06
DEV = pl.DeviceIdType.MESH

OFFSETS = (
    (0, 0), (1, 1), (3, 3), (0, 1), (0, 3), (2, 2), (1, 3), (3, 1),
    (1, 0), (3, 0), (2, 1), (2, 3), (1, 2), (3, 2), (0, 2), (2, 0),
)
SLOT_OF = {0: 0, 1: 1, -1: 2, 2: 3, -2: 4, 3: 5, -3: 6, 4: 7, -4: 7}
CW, CCW = 0, 1


phase = jax.named_scope


def wait_for(ref, sem):
    pltpu.make_async_copy(ref, ref, sem).wait()


def kernel(
    gate_hbm, up_hbm, down_hbm, mix_hbm, pool_hbm, x_hbm,
    pool_gain, moe_gain, ids_ref, route_ref,
    mixed_ref, moe_ref,
    w_in, w_down, w_mix, w_plane,
    pool_in, halo, pooled, pooled_all, x_in, normed, placing, picking,
    outgoing, arrived, hidden, rows_out, rows_back, pooled_rows, mixed_sum,
    load_sem, ring_recv, ring_send, push_send, sib_in, sib_down, sib_mix, plane_send, plane_recv,
    disp_send, disp_recv, halo_sem, pool_sem, ret_send, ret_recv,
):
    ep = lax.axis_index("ep")
    tp = lax.axis_index("tp")
    px, py = lax.rem(ep, NX), ep // NX
    pz, core = tp // 2, lax.rem(tp, 2)

    def plane(dx, dy):
        return (lax.rem(py + dy, NY) * NX + lax.rem(px + dx, NX), tp)

    def column(dz, dc):
        return (ep, lax.rem(pz + dz, NZ) * 2 + lax.rem(core + dc, 2))

    sibling = column(0, 1)
    ring_to = {CW: column(1, 0), CCW: column(NZ - 1, 0)}

    barrier = pltpu.get_barrier_semaphore()
    for dx, dy in OFFSETS[1:]:
        pl.semaphore_signal(barrier, inc=1, device_id=plane(dx, dy), device_id_type=DEV)
    for dz in range(NZ):
        for dc in range(2):
            if (dz, dc) != (0, 0):
                pl.semaphore_signal(barrier, inc=1, device_id=column(dz, dc), device_id_type=DEV)

    def piece(ref, index=None):
        def at(slot, other):
            rows = pl.ds(slot * 128 + 64 * other, 64)
            return ref.at[rows] if index is None else ref.at[index, rows]

        return at

    pieces = {
        "g": lambda slot, other: w_in.at[slot, pl.ds(64 * other, 64)],
        "u": lambda slot, other: w_in.at[slot, pl.ds(128 + 64 * other, 64)],
    }
    hops = {"g": (4, 3), "u": (3, 4)}
    for q in range(4):
        pieces[f"d{q}"] = piece(w_down, q)
        hops[f"d{q}"] = (4, 3) if q % 2 == 0 else (3, 4)
    for h in range(2):
        pieces[f"m{h}"] = piece(w_mix, h)
        hops[f"m{h}"] = (4, 3) if h == 0 else (3, 4)
    names = list(pieces)
    number = {name: k for k, name in enumerate(names)}

    loads = {}

    def load(name, src, dst):
        copy = pltpu.make_async_copy(src, dst, load_sem.at[len(loads)])
        copy.start()
        loads[name] = copy

    load("g", gate_hbm, w_in.at[0, pl.ds(0, 64)])
    load("u", up_hbm, w_in.at[0, pl.ds(128, 64)])
    load("d0", down_hbm.at[:, pl.ds(0, 512)], w_down.at[0, pl.ds(0, 64)])
    load("x", x_hbm, x_in)
    load("pool", pool_hbm, pool_in)
    for q in range(1, 4):
        load(f"d{q}", down_hbm.at[:, pl.ds(512 * q, 512)], w_down.at[q, pl.ds(0, 64)])
    for h in range(2):
        load(f"m{h}", mix_hbm.at[:, pl.ds(1024 + 512 * h, 512)], w_mix.at[h, pl.ds(0, 64)])
    load("plane", mix_hbm.at[:, pl.ds(0, 1024)], w_plane.at[0, pl.ds(0, 64)])

    def sib_sem(name, slot):
        if name in "gu":
            return sib_in.at[number[name], (0, 0, 0, 1, 1, 2, 2, 3)[slot]]
        if name[0] == "d":
            return sib_down.at[int(name[1])]
        return sib_mix.at[int(name[1]), slot // 7]

    def ring_copy(name, way, hop):
        sign = -1 if way == CW else 1
        source, target = SLOT_OF[sign * (hop - 1)], SLOT_OF[sign * hop]
        at = pieces[name]
        return pltpu.make_async_remote_copy(
            src_ref=at(source, 0),
            dst_ref=at(target, 0),
            send_sem=ring_send.at[number[name]],
            recv_sem=ring_recv.at[number[name], way * 4 + hop - 1],
            device_id=ring_to[way],
            device_id_type=DEV,
        )

    def last_copy(name, half):
        way = CW if name == "g" else CCW
        at, rows = pieces[name], pl.ds(32 * half, 32)
        source = SLOT_OF[-3 if way == CW else 3]
        return pltpu.make_async_remote_copy(
            src_ref=at(source, 0).at[rows],
            dst_ref=at(SLOT_OF[4], 0).at[rows],
            send_sem=ring_send.at[number[name]],
            recv_sem=ring_recv.at[number[name], 3 + 4 * half],
            device_id=ring_to[way],
            device_id_type=DEV,
        )

    def push(name, slot, rows=slice(None)):
        at = pieces[name]
        pltpu.make_async_remote_copy(
            src_ref=at(slot, 0).at[rows],
            dst_ref=at(slot, 1).at[rows],
            send_sem=push_send.at[number[name]],
            recv_sem=sib_sem(name, slot),
            device_id=sibling,
            device_id_type=DEV,
        ).start()

    def first_sends(*pairs):
        for name, way in pairs:
            ring_copy(name, way, 1).start()

    def arrival(name, way, hop):
        if hop > hops[name][way]:
            return
        ring_copy(name, way, hop).wait_recv()
        if hop < hops[name][way]:
            if name in "gu" and hop == 3:
                last_copy(name, 0).start()
                last_copy(name, 1).start()
            else:
                ring_copy(name, way, hop + 1).start()
        push(name, SLOT_OF[-hop if way == CW else hop])

    def arrivals(hop, *pairs):
        for name, way in pairs:
            arrival(name, way, hop)

    set_one = (("g", CW), ("u", CCW), ("u", CW), ("g", CCW), ("d0", CW), ("d0", CCW))
    set_mix = (("m0", CW), ("m1", CCW), ("m1", CW), ("m0", CCW))

    def both(name):
        return ((name, CCW), (name, CW))

    def plane_copy(number, source, target, device):
        return pltpu.make_async_remote_copy(
            src_ref=source,
            dst_ref=target,
            send_sem=plane_send.at[number],
            recv_sem=plane_recv.at[number],
            device_id=device,
            device_id_type=DEV,
        )

    def x_part(at_x, first, count):
        rows = pl.ds(pl.multiple_of(lax.rem(at_x, 2) * 32, 32), 32)
        cols = pl.ds(pl.multiple_of((2 * py + at_x // 2) * 128, 128), 128)
        return w_plane.at[pl.ds(first, count), rows, cols]

    def y_part(at_y, first, count):
        cols = pl.ds(pl.multiple_of(at_y * 256, 256), 256)
        return w_plane.at[pl.ds(first, count), pl.ds(0, 64), cols]

    x_own, y_own = x_part(px, 1, 7), y_part(py, 1, 7)
    x_copies = [plane_copy(k, x_own, x_own, plane((0, 1, NX - 1, 2)[k], 0)) for k in (1, 2, 3)]
    y_copies = [plane_copy(3 + k, y_own, y_own, plane(0, (0, 1, NY - 1, 2)[k])) for k in (1, 2, 3)]

    def z_copy(dz):
        rel = -dz if dz <= 4 else NZ - dz
        own = x_part(px, 0, 1)
        return plane_copy(0, own, x_part(px, SLOT_OF[rel], 1), column(dz, 0))

    plane_pushes = [
        plane_copy(
            7 + k,
            w_plane.at[pl.ds(k, (1, 7)[k]), pl.ds(0, 64)],
            w_plane.at[pl.ds(k, (1, 7)[k]), pl.ds(64, 64)],
            sibling,
        )
        for k in range(2)
    ]
    z_bytes = w_plane.at[pl.ds(1, 7), pl.ds(0, 32), pl.ds(0, 128)]

    with phase("enter"):
        pl.semaphore_wait(barrier, 30)
    with phase("first"):
        loads["g"].wait()
        first_sends(("g", CW))
        loads["u"].wait()
        first_sends(*set_one[1:4])
        loads["d0"].wait()
        first_sends(*set_one[4:])

    loads["pool"].wait()
    halo_copy = pltpu.make_async_remote_copy(
        src_ref=pool_in.at[:, pl.ds(pool_in.shape[1] - 128, 128)],
        dst_ref=halo,
        send_sem=halo_sem.at[0],
        recv_sem=halo_sem.at[1],
        device_id=(lax.rem(ep + 1, EXPERTS), tp),
        device_id_type=DEV,
    )
    halo_copy.start()

    for name in ("g", "u", "d0"):
        push(name, 0)

    loads["x"].wait()
    gain_row = moe_gain[...]

    def norm_rows(k, carry):
        rows = pl.ds(k * 64, 64)
        v = x_in[rows, :].astype(jnp.float32)
        scale = lax.rsqrt(jnp.mean(v * v, axis=-1, keepdims=True) + EPS_NORM)
        normed[rows, :] = (v * scale * gain_row).astype(jnp.bfloat16)
        return carry

    with phase("norm"):
        lax.fori_loop(0, 4, norm_rows, 0)

    tokens = x_in.shape[0]
    expert = lax.broadcasted_iota(jnp.int32, (EXPERTS, tokens), 0)
    ids = ids_ref[...]
    chosen = [(ids[k : k + 1, :] == expert).astype(jnp.float32) for k in range(2)]
    marked = (chosen[0] + chosen[1]).astype(jnp.bfloat16)
    before = (
        lax.broadcasted_iota(jnp.int32, (tokens, tokens), 0)
        < lax.broadcasted_iota(jnp.int32, (tokens, tokens), 1)
    ).astype(jnp.bfloat16)
    rank = jnp.dot(marked, before, preferred_element_type=jnp.float32)
    away = lax.rem(expert // NX - py + NY, NY) * NX + lax.rem(lax.rem(expert, NX) - px + NX, NX)
    place = jnp.zeros((EXPERTS, tokens), jnp.float32)
    for p, (dx, dy) in enumerate(OFFSETS):
        place = jnp.where(away == dy * NX + dx, float(p * CAP), place)
    slot_of = place + rank
    slots = [
        jnp.sum(chosen[k] * slot_of, axis=0, keepdims=True).astype(jnp.int32) for k in range(2)
    ]

    def disp_copy(p):
        dx, dy = OFFSETS[p]
        rows = pl.ds(p * CAP, CAP)
        return pltpu.make_async_remote_copy(
            src_ref=outgoing.at[rows],
            dst_ref=arrived.at[rows],
            send_sem=disp_send,
            recv_sem=disp_recv.at[p // 8],
            device_id=plane(dx, dy),
            device_id_type=DEV,
        )

    for group in range(4):
        row_ids = lax.broadcasted_iota(jnp.int32, (4 * CAP, tokens), 0) + group * 4 * CAP
        hit = (row_ids == slots[0]) | (row_ids == slots[1])
        placing[...] = hit.astype(jnp.bfloat16)

        def place_columns(n, carry, group=group):
            cols = pl.ds(pl.multiple_of(n * 512, 512), 512)
            block = jnp.dot(
                placing[...], normed[:, cols], preferred_element_type=jnp.float32
            ).astype(jnp.bfloat16)
            outgoing[pl.ds(group * 4 * CAP, 4 * CAP), cols] = block
            if group == 0:
                arrived[pl.ds(0, CAP), cols] = block[:CAP]
            return carry

        lax.fori_loop(0, 4, place_columns, 0)
        if group < 2:
            for p in range(max(1, group * 4), group * 4 + 4):
                disp_copy(p).start()

    loads["plane"].wait()
    for dz in (4, 3, 5, 2, 6, 1, 7):
        z_copy(dz).start()
    plane_pushes[0].start()
    with phase("one_1"):
        arrivals(1, *set_one)
    loads["d1"].wait()
    first_sends(*both("d1"))
    push("d1", 0)

    route = route_ref[...]
    slot_rows = lax.broadcasted_iota(jnp.int32, (EXPERTS * CAP, tokens), 0)
    weighted = jnp.where(slot_rows == slots[0], route[0:1, :], 0.0) + jnp.where(
        slot_rows == slots[1], route[1:2, :], 0.0
    )
    picking[...] = weighted.T.astype(jnp.bfloat16)

    with phase("halo"):
        halo_copy.wait_recv()
    row_count = pool_in.shape[1]
    window_group = (tp * 64) // GROUP_CH
    gain_wide = pool_gain[...]
    diagonal = lax.broadcasted_iota(jnp.int32, (64, 64), 0) == lax.broadcasted_iota(
        jnp.int32, (64, 64), 1
    )
    gain_col = jnp.sum(jnp.where(diagonal, gain_wide, 0.0), axis=1, keepdims=True)
    for part in range(4):
        r = slice(part * 16, part * 16 + 16)
        values = pool_in[r, :].astype(jnp.float32)
        carried = jnp.where(ep > 0, halo[r, :].astype(jnp.float32), 0.0)
        level = jnp.concatenate([carried, values], axis=1)
        summed = jnp.zeros_like(values)
        for doubling in range(4):
            level = level + pltpu.roll(level, 2**doubling, 1)
            summed = jnp.where(window_group == doubling, level[:, 128:], summed)
        position = ep * row_count + lax.broadcasted_iota(jnp.int32, (1, row_count), 1)
        width = 2 ** 1
        for doubling in range(1, 4):
            width = jnp.where(window_group == doubling, 2 ** (doubling + 1), width)
        counted = jnp.minimum(position + 1, width).astype(jnp.float32)
        pooled[r, :] = ((summed / counted - values) * gain_col[r, :]).astype(jnp.bfloat16)
    pooled_all[pl.ds(0, 64), :] = pooled[:, pl.ds(pl.multiple_of(tp * 128, 128), 128)]

    def pool_copy(dz, dc):
        target = lax.rem(pz + dz, NZ) * 2 + lax.rem(core + dc, 2)
        rel = -dz if dz <= 4 else NZ - dz
        return pltpu.make_async_remote_copy(
            src_ref=pooled.at[:, pl.ds(pl.multiple_of(target * 128, 128), 128)],
            dst_ref=pooled_all.at[pl.ds(SLOT_OF[rel] * 128 + 64 * dc, 64)],
            send_sem=pool_sem.at[0],
            recv_sem=pool_sem.at[1],
            device_id=column(dz, dc),
            device_id_type=DEV,
        )

    half_rows = 8 * CAP

    def gated(both_parts):
        gate_part, upward = both_parts[:, :128], both_parts[:, 128:]
        return (gate_part / (1.0 + jnp.exp(-gate_part)) * upward).astype(jnp.bfloat16)

    def project(rows, weights):
        return lax.dot_general(
            arrived[rows, :], weights, (((1,), (1,)), ((), ())), preferred_element_type=jnp.float32
        )

    def hidden_pairs(half, first_slot, pairs):
        rows = pl.ds(half * half_rows, half_rows)

        def one(pair, carry):
            slot = first_slot + 2 * pair
            sums = project(rows, w_in[pl.ds(slot, 2)].reshape(512, w_in.shape[2]))
            for k in range(2):
                cols = pl.ds(pl.multiple_of((slot + k) * 128, 128), 128)
                hidden[rows, cols] = gated(sums[:, 256 * k : 256 * k + 256])
            return carry

        lax.fori_loop(0, pairs, one, 0)

    def ret_copy(q, p):
        dx, dy = OFFSETS[p]
        rows = pl.ds(p * CAP, CAP)
        return pltpu.make_async_remote_copy(
            src_ref=rows_out.at[q, rows],
            dst_ref=rows_back.at[q, rows],
            send_sem=ret_send.at[q],
            recv_sem=ret_recv.at[q],
            device_id=plane(NX - dx, NY - dy),
            device_id_type=DEV,
        )

    def give_back(q, half):
        rows = pl.ds(half * half_rows, half_rows)
        block = jnp.dot(
            hidden[rows, :], w_down[q], preferred_element_type=jnp.float32
        ).astype(jnp.bfloat16)
        rows_out[q, rows] = block
        if half == 0:
            rows_back[q, pl.ds(0, CAP)] = block[:CAP]
        for p in range(max(1, half * 8), half * 8 + 8):
            ret_copy(q, p).start()

    def combine(q):
        wait_for(rows_back.at[q, pl.ds(CAP, 15 * CAP)], ret_recv.at[q])
        moe_ref[:, pl.ds(q * 512, 512)] = jnp.dot(
            picking[...], rows_back[q], preferred_element_type=jnp.float32
        ).astype(jnp.bfloat16)

    def down_ready(q):
        wait_for(w_down.at[q, pl.ds(0, 512)], sib_down.at[q])

    def in_ready(hop):
        for part in range(2):
            if hop == 1:
                wait_for(arrived.at[pl.ds(0, 192)], sib_in.at[part, 0])
            else:
                wait_for(w_in.at[0, pl.ds(0, 64 if hop == 4 else 128)], sib_in.at[part, hop - 1])

    with phase("in_1"):
        in_ready(1)
    for p in range(8, 16):
        disp_copy(p).start()
    with phase("one_2a"):
        arrivals(2, *set_one[:2])
    with phase("plane_z"):
        wait_for(z_bytes, plane_recv.at[0])
    for copy in x_copies:
        copy.start()
    with phase("one_2b"):
        arrivals(2, *set_one[2:])
    with phase("d1_1"):
        arrivals(1, *both("d1"))
    with phase("disp_0"):
        wait_for(arrived.at[pl.ds(CAP, 7 * CAP)], disp_recv.at[0])
        in_ready(2)
    with phase("hid_a"):
        hidden_pairs(0, 0, 2)
    with phase("one_3"):
        arrivals(3, *set_one)
    with phase("plane_x"):
        for copy in x_copies:
            copy.wait_recv()
    for copy in y_copies:
        copy.start()
    with phase("in_3"):
        in_ready(3)
    with phase("hid_b"):
        hidden_pairs(0, 4, 1)
    with phase("d1_2"):
        arrivals(2, *both("d1"))
    for q in (2, 3):
        loads[f"d{q}"].wait()
        first_sends(*both(f"d{q}"))
        push(f"d{q}", 0)
    with phase("disp_1"):
        wait_for(arrived.at[pl.ds(8 * CAP, 8 * CAP)], disp_recv.at[1])
    with phase("hid_c"):
        hidden_pairs(1, 0, 3)
    with phase("one_4"):
        for half in range(2):
            for name in "gu":
                last_copy(name, half).wait_recv()
                push(name, SLOT_OF[4], pl.ds(32 * half, 32))
    with phase("one_4d"):
        arrivals(4, *set_one[4:])
    with phase("in_4"):
        in_ready(4)
    with phase("hid_67a"):
        hidden_pairs(0, 6, 1)
    with phase("d0"):
        down_ready(0)
    with phase("give_0a"):
        give_back(0, 0)
    with phase("hid_67b"):
        hidden_pairs(1, 6, 1)
    with phase("give_0b"):
        give_back(0, 1)
    with phase("two_1"):
        arrivals(3, *both("d1"))
        arrivals(1, *both("d2"))
        arrivals(1, *both("d3"))
    with phase("two_2"):
        arrivals(4, *both("d1"))
        arrivals(2, *both("d2"))
        down_ready(1)
    with phase("give_1a"):
        give_back(1, 0)
    with phase("two_2b"):
        arrivals(2, *both("d3"))
    for copy in y_copies:
        copy.wait_recv()
    plane_pushes[1].start()
    with phase("give_1b"):
        give_back(1, 1)
    with phase("two_3"):
        arrivals(3, *both("d2"))
    for h in range(2):
        loads[f"m{h}"].wait()
    with phase("two_3b"):
        arrivals(3, *both("d3"))
    first_sends(*set_mix)
    for h in range(2):
        push(f"m{h}", 0)
    for dz in (4, 3, 5, 2, 6, 1, 7, 0):
        for dc in range(2):
            if (dz, dc) != (0, 0):
                pool_copy(dz, dc).start()
    with phase("two_4"):
        arrivals(4, *both("d2"))
        arrivals(4, *both("d3"))
    with phase("d2"):
        down_ready(2)
    with phase("give_2"):
        give_back(2, 0)
        give_back(2, 1)
    with phase("d3"):
        down_ready(3)
    with phase("give_3"):
        give_back(3, 0)
        give_back(3, 1)
    with phase("mix_1"):
        arrivals(1, *set_mix)
    with phase("combine_0"):
        combine(0)
    with phase("mix_2"):
        arrivals(2, *set_mix)
    with phase("combine_1"):
        combine(1)
    with phase("pool_wait"):
        wait_for(pooled_all.at[pl.ds(64, 960)], pool_sem.at[1])
    pooled_rows[...] = pooled_all[...].astype(jnp.float32).T.astype(jnp.bfloat16)
    with phase("mix_3"):
        arrivals(3, *set_mix)

    with phase("mixer_0"):
        for push_copy in plane_pushes:
            push_copy.wait_recv()
        for cols in (pl.ds(0, 512), pl.ds(512, 512)):
            mixed_ref[:, cols] = jnp.dot(
                pooled_rows[...],
                w_plane[:, :, cols].reshape(1024, 512),
                preferred_element_type=jnp.float32,
            ).astype(jnp.bfloat16)
    for h in range(2):
        wait_for(w_mix.at[h, pl.ds(0, 448)], sib_mix.at[h, 0])
    with phase("mixer"):
        for h in range(2):
            mixed_sum[h] = jnp.dot(
                pooled_rows[:, :896], w_mix[h, :896], preferred_element_type=jnp.float32
            )
    with phase("combine_2"):
        combine(2)
    with phase("mix_4"):
        arrivals(4, *set_mix)
        for h in range(2):
            wait_for(w_mix.at[h, pl.ds(0, 64)], sib_mix.at[h, 1])
    with phase("mixer_2"):
        for h in range(2):
            last = jnp.dot(pooled_rows[:, 896:], w_mix[h, 896:], preferred_element_type=jnp.float32)
            mixed_ref[:, pl.ds(1024 + h * 512, 512)] = (mixed_sum[h] + last).astype(jnp.bfloat16)
    for name in names:
        if name in "gu":
            sent, pushed = outgoing.at[pl.ds(0, 7 * 64)], outgoing.at[pl.ds(0, 8 * 64)]
        else:
            whole = w_down.at[int(name[1])] if name[0] == "d" else w_mix.at[int(name[1])]
            sent, pushed = whole.at[pl.ds(0, 7 * 64)], whole.at[pl.ds(0, 8 * 64)]
        wait_for(sent, ring_send.at[number[name]])
        wait_for(pushed, push_send.at[number[name]])
    wait_for(outgoing.at[pl.ds(CAP, 15 * CAP)], disp_send)
    halo_copy.wait_send()
    wait_for(z_bytes, plane_send.at[0])
    for copy in (*x_copies, *y_copies, *plane_pushes):
        copy.wait_send()
    wait_for(pooled_all.at[pl.ds(64, 960)], pool_sem.at[0])
    for q in range(3):
        wait_for(rows_out.at[q, pl.ds(CAP, 15 * CAP)], ret_send.at[q])
    with phase("combine_3"):
        combine(3)
    with phase("end"):
        wait_for(rows_out.at[3, pl.ds(CAP, 15 * CAP)], ret_send.at[3])


def body(
    pool_input,
    pool_gain,
    mix_weight,
    moe_input,
    moe_gain,
    expert_ids,
    route_weight,
    gate_weight,
    up_weight,
    down_weight,
):
    rows_a, channels = pool_input.shape
    tokens, width = moe_input.shape
    slots = EXPERTS * CAP
    bf, f32 = jnp.bfloat16, jnp.float32
    hbm = pl.BlockSpec(memory_space=pl.ANY)
    vmem = pl.BlockSpec(memory_space=pltpu.VMEM)
    dma = pltpu.SemaphoreType.DMA
    return pl.pallas_call(
        kernel,
        out_shape=(
            pltpu.VMEM((rows_a // 16, width), bf),
            pltpu.VMEM((tokens, width), bf),
        ),
        in_specs=[hbm] * 6 + [vmem] * 4,
        out_specs=(vmem, vmem),
        scratch_shapes=[
            pltpu.VMEM((8, 256, width), bf),
            pltpu.VMEM((4, 1024, 512), bf),
            pltpu.VMEM((2, 1024, 512), bf),
            pltpu.VMEM((8, 128, 1024), bf),
            pltpu.VMEM((channels, rows_a), bf),
            pltpu.VMEM((channels, 128), bf),
            pltpu.VMEM((channels, rows_a), bf),
            pltpu.VMEM((1024, 128), bf),
            pltpu.VMEM((tokens, width), bf),
            pltpu.VMEM((tokens, width), bf),
            pltpu.VMEM((4 * CAP, tokens), bf),
            pltpu.VMEM((tokens, slots), bf),
            pltpu.VMEM((slots, width), bf),
            pltpu.VMEM((slots, width), bf),
            pltpu.VMEM((slots, 1024), bf),
            pltpu.VMEM((4, slots, 512), bf),
            pltpu.VMEM((4, slots, 512), bf),
            pltpu.VMEM((rows_a // 16, 1024), bf),
            pltpu.VMEM((2, rows_a // 16, 512), f32),
            dma((11,)),
            dma((8, 8)),
            dma((8,)),
            dma((8,)),
            dma((2, 4)),
            dma((4,)),
            dma((2, 2)),
            dma((11,)),
            dma((11,)),
            dma,
            dma((2,)),
            dma((2,)),
            dma((2,)),
            dma((4,)),
            dma((4,)),
        ],
        compiler_params=pltpu.CompilerParams(
            collective_id=0, has_side_effects=True, vmem_limit_bytes=56 << 20
        ),
        name="mixer_and_experts",
    )(
        gate_weight[0].T,
        up_weight[0].T,
        down_weight[0].T,
        mix_weight,
        pool_input.T,
        moe_input,
        pool_gain.reshape(1, channels),
        moe_gain.reshape(1, width),
        expert_ids.T,
        route_weight.T,
    )


def solution(mesh):
    return jax.shard_map(
        body,
        mesh=mesh,
        in_specs=(
            P("ep", "tp"),
            P("tp"),
            P("tp", None),
            P(("ep", "tp"), None),
            P(),
            P(("ep", "tp"), None),
            P(("ep", "tp"), None),
            P("ep", None, "tp"),
            P("ep", None, "tp"),
            P("ep", None, "tp"),
        ),
        out_specs=(P(("ep", "tp"), None), P(("ep", "tp"), None)),
        check_vma=False,
    )
```

```python
import functools

import jax
import jax.numpy as jnp
from jax import lax
from jax.experimental import pallas as pl
from jax.experimental.pallas import tpu as pltpu
from jax.sharding import PartitionSpec as P

GROUP_CH = 256
EXPERTS = 16
CAP = 48
NX, NY, NZ = 4, 4, 8
EPS_NORM = 1e-06
DEV = pl.DeviceIdType.MESH

OFFSETS = (
    (0, 0), (1, 1), (3, 3), (0, 1), (0, 3), (2, 2), (1, 3), (3, 1),
    (1, 0), (3, 0), (2, 1), (2, 3), (1, 2), (3, 2), (0, 2), (2, 0),
)
SLOT_OF = {0: 0, 1: 1, -1: 2, 2: 3, -2: 4, 3: 5, -3: 6, 4: 7, -4: 7}
CW, CCW = 0, 1


phase = jax.named_scope


def wait_for(ref, sem):
    pltpu.make_async_copy(ref, ref, sem).wait()


def kernel(
    gate_hbm, up_hbm, down_hbm, mix_hbm, pool_hbm, x_hbm,
    pool_gain_hbm, moe_gain_hbm, ids_hbm, route_hbm,
    mixed_ref, moe_ref,
    w_in, w_down, w_mix, w_plane,
    pool_in, halo, pooled, pooled_all, x_in, normed, placing, picking,
    outgoing, arrived, hidden, rows_out, rows_back, pooled_rows, mixed_sum,
    pool_gain, moe_gain, ids_ref, route_ref,
    load_sem, ring_recv, ring_send, push_send, sib_in, sib_down, sib_mix, plane_send, plane_recv,
    disp_send, disp_recv, halo_sem, pool_sem, ret_send, ret_recv,
):
    ep = lax.axis_index("ep")
    tp = lax.axis_index("tp")
    px, py = lax.rem(ep, NX), ep // NX
    pz, core = tp // 2, lax.rem(tp, 2)

    def plane(dx, dy):
        return (lax.rem(py + dy, NY) * NX + lax.rem(px + dx, NX), tp)

    def column(dz, dc):
        return (ep, lax.rem(pz + dz, NZ) * 2 + lax.rem(core + dc, 2))

    sibling = column(0, 1)
    ring_to = {CW: column(1, 0), CCW: column(NZ - 1, 0)}

    barrier = pltpu.get_barrier_semaphore()
    for dx, dy in OFFSETS[1:]:
        pl.semaphore_signal(barrier, inc=1, device_id=plane(dx, dy), device_id_type=DEV)
    for dz in range(NZ):
        for dc in range(2):
            if (dz, dc) != (0, 0):
                pl.semaphore_signal(barrier, inc=1, device_id=column(dz, dc), device_id_type=DEV)

    def piece(ref, index=None):
        def at(slot, other):
            rows = pl.ds(slot * 128 + 64 * other, 64)
            return ref.at[rows] if index is None else ref.at[index, rows]

        return at

    pieces = {
        "g": lambda slot, other: w_in.at[slot, pl.ds(64 * other, 64)],
        "u": lambda slot, other: w_in.at[slot, pl.ds(128 + 64 * other, 64)],
    }
    hops = {"g": (4, 3), "u": (3, 4)}
    for q in range(4):
        pieces[f"d{q}"] = piece(w_down, q)
        hops[f"d{q}"] = (4, 3) if q % 2 == 0 else (3, 4)
    for h in range(2):
        pieces[f"m{h}"] = piece(w_mix, h)
        hops[f"m{h}"] = (4, 3) if h == 0 else (3, 4)
    names = list(pieces)
    number = {name: k for k, name in enumerate(names)}

    loads = {}

    def load(name, src, dst):
        copy = pltpu.make_async_copy(src, dst, load_sem.at[len(loads)])
        copy.start()
        loads[name] = copy

    load("g", gate_hbm, w_in.at[0, pl.ds(0, 64)])
    load("u", up_hbm, w_in.at[0, pl.ds(128, 64)])
    load("d0", down_hbm.at[:, pl.ds(0, 512)], w_down.at[0, pl.ds(0, 64)])
    load("x", x_hbm, x_in)
    load("ids", ids_hbm, ids_ref)
    load("moe_gain", moe_gain_hbm, moe_gain)
    load("route", route_hbm, route_ref)
    load("pool_gain", pool_gain_hbm, pool_gain)
    load("pool", pool_hbm, pool_in)
    for q in range(1, 4):
        load(f"d{q}", down_hbm.at[:, pl.ds(512 * q, 512)], w_down.at[q, pl.ds(0, 64)])
    for h in range(2):
        load(f"m{h}", mix_hbm.at[:, pl.ds(1024 + 512 * h, 512)], w_mix.at[h, pl.ds(0, 64)])
    load("plane", mix_hbm.at[:, pl.ds(0, 1024)], w_plane.at[0, pl.ds(0, 64)])

    def sib_sem(name, slot):
        if name in "gu":
            return sib_in.at[number[name], (0, 0, 0, 1, 1, 2, 2, 3)[slot]]
        if name[0] == "d":
            return sib_down.at[int(name[1])]
        return sib_mix.at[int(name[1]), slot // 7]

    def ring_copy(name, way, hop):
        sign = -1 if way == CW else 1
        source, target = SLOT_OF[sign * (hop - 1)], SLOT_OF[sign * hop]
        at = pieces[name]
        return pltpu.make_async_remote_copy(
            src_ref=at(source, 0),
            dst_ref=at(target, 0),
            send_sem=ring_send.at[number[name]],
            recv_sem=ring_recv.at[number[name], way * 4 + hop - 1],
            device_id=ring_to[way],
            device_id_type=DEV,
        )

    def last_copy(name, half):
        way = CW if name == "g" else CCW
        at, rows = pieces[name], pl.ds(32 * half, 32)
        source = SLOT_OF[-3 if way == CW else 3]
        return pltpu.make_async_remote_copy(
            src_ref=at(source, 0).at[rows],
            dst_ref=at(SLOT_OF[4], 0).at[rows],
            send_sem=ring_send.at[number[name]],
            recv_sem=ring_recv.at[number[name], 3 + 4 * half],
            device_id=ring_to[way],
            device_id_type=DEV,
        )

    def push(name, slot, rows=slice(None)):
        at = pieces[name]
        pltpu.make_async_remote_copy(
            src_ref=at(slot, 0).at[rows],
            dst_ref=at(slot, 1).at[rows],
            send_sem=push_send.at[number[name]],
            recv_sem=sib_sem(name, slot),
            device_id=sibling,
            device_id_type=DEV,
        ).start()

    def first_sends(*pairs):
        for name, way in pairs:
            ring_copy(name, way, 1).start()

    def arrival(name, way, hop):
        if hop > hops[name][way]:
            return
        ring_copy(name, way, hop).wait_recv()
        if hop < hops[name][way]:
            if name in "gu" and hop == 3:
                last_copy(name, 0).start()
                last_copy(name, 1).start()
            else:
                ring_copy(name, way, hop + 1).start()
        push(name, SLOT_OF[-hop if way == CW else hop])

    def arrivals(hop, *pairs):
        for name, way in pairs:
            arrival(name, way, hop)

    set_one = (("g", CW), ("u", CCW), ("u", CW), ("g", CCW), ("d0", CW), ("d0", CCW))
    set_mix = (("m0", CW), ("m1", CCW), ("m1", CW), ("m0", CCW))

    def both(name):
        return ((name, CCW), (name, CW))

    def plane_copy(number, source, target, device):
        return pltpu.make_async_remote_copy(
            src_ref=source,
            dst_ref=target,
            send_sem=plane_send.at[number],
            recv_sem=plane_recv.at[number],
            device_id=device,
            device_id_type=DEV,
        )

    def x_part(at_x, first, count):
        rows = pl.ds(pl.multiple_of(lax.rem(at_x, 2) * 32, 32), 32)
        cols = pl.ds(pl.multiple_of((2 * py + at_x // 2) * 128, 128), 128)
        return w_plane.at[pl.ds(first, count), rows, cols]

    def y_part(at_y, first, count):
        cols = pl.ds(pl.multiple_of(at_y * 256, 256), 256)
        return w_plane.at[pl.ds(first, count), pl.ds(0, 64), cols]

    x_own, y_own = x_part(px, 1, 7), y_part(py, 1, 7)
    x_copies = [plane_copy(k, x_own, x_own, plane((0, 1, NX - 1, 2)[k], 0)) for k in (1, 2, 3)]
    y_copies = [plane_copy(3 + k, y_own, y_own, plane(0, (0, 1, NY - 1, 2)[k])) for k in (1, 2, 3)]

    def z_copy(dz):
        rel = -dz if dz <= 4 else NZ - dz
        own = x_part(px, 0, 1)
        return plane_copy(0, own, x_part(px, SLOT_OF[rel], 1), column(dz, 0))

    plane_pushes = [
        plane_copy(
            7 + k,
            w_plane.at[pl.ds(k, (1, 7)[k]), pl.ds(0, 64)],
            w_plane.at[pl.ds(k, (1, 7)[k]), pl.ds(64, 64)],
            sibling,
        )
        for k in range(2)
    ]
    z_bytes = w_plane.at[pl.ds(1, 7), pl.ds(0, 32), pl.ds(0, 128)]

    with phase("enter"):
        pl.semaphore_wait(barrier, 30)
    with phase("first"):
        loads["g"].wait()
        first_sends(("g", CW))
        loads["u"].wait()
        first_sends(*set_one[1:4])
        loads["d0"].wait()
        first_sends(*set_one[4:])

    loads["pool"].wait()
    halo_copy = pltpu.make_async_remote_copy(
        src_ref=pool_in.at[:, pl.ds(pool_in.shape[1] - 128, 128)],
        dst_ref=halo,
        send_sem=halo_sem.at[0],
        recv_sem=halo_sem.at[1],
        device_id=(lax.rem(ep + 1, EXPERTS), tp),
        device_id_type=DEV,
    )
    halo_copy.start()

    for name in ("g", "u", "d0"):
        push(name, 0)

    for name in ("x", "ids", "moe_gain", "route", "pool_gain"):
        loads[name].wait()
    gain_row = moe_gain[...]

    def norm_rows(k, carry):
        rows = pl.ds(k * 64, 64)
        v = x_in[rows, :].astype(jnp.float32)
        scale = lax.rsqrt(jnp.mean(v * v, axis=-1, keepdims=True) + EPS_NORM)
        normed[rows, :] = (v * scale * gain_row).astype(jnp.bfloat16)
        return carry

    with phase("norm"):
        lax.fori_loop(0, 4, norm_rows, 0)

    tokens = x_in.shape[0]
    expert = lax.broadcasted_iota(jnp.int32, (EXPERTS, tokens), 0)
    ids = ids_ref[...]
    chosen = [(ids[k : k + 1, :] == expert).astype(jnp.float32) for k in range(2)]
    marked = (chosen[0] + chosen[1]).astype(jnp.bfloat16)
    before = (
        lax.broadcasted_iota(jnp.int32, (tokens, tokens), 0)
        < lax.broadcasted_iota(jnp.int32, (tokens, tokens), 1)
    ).astype(jnp.bfloat16)
    rank = jnp.dot(marked, before, preferred_element_type=jnp.float32)
    away = lax.rem(expert // NX - py + NY, NY) * NX + lax.rem(lax.rem(expert, NX) - px + NX, NX)
    place = jnp.zeros((EXPERTS, tokens), jnp.float32)
    for p, (dx, dy) in enumerate(OFFSETS):
        place = jnp.where(away == dy * NX + dx, float(p * CAP), place)
    slot_of = place + rank
    slots = [
        jnp.sum(chosen[k] * slot_of, axis=0, keepdims=True).astype(jnp.int32) for k in range(2)
    ]

    def disp_copy(p):
        dx, dy = OFFSETS[p]
        rows = pl.ds(p * CAP, CAP)
        return pltpu.make_async_remote_copy(
            src_ref=outgoing.at[rows],
            dst_ref=arrived.at[rows],
            send_sem=disp_send,
            recv_sem=disp_recv.at[p // 8],
            device_id=plane(dx, dy),
            device_id_type=DEV,
        )

    for group in range(4):
        row_ids = lax.broadcasted_iota(jnp.int32, (4 * CAP, tokens), 0) + group * 4 * CAP
        hit = (row_ids == slots[0]) | (row_ids == slots[1])
        placing[...] = hit.astype(jnp.bfloat16)

        def place_columns(n, carry, group=group):
            cols = pl.ds(pl.multiple_of(n * 512, 512), 512)
            block = jnp.dot(
                placing[...], normed[:, cols], preferred_element_type=jnp.float32
            ).astype(jnp.bfloat16)
            outgoing[pl.ds(group * 4 * CAP, 4 * CAP), cols] = block
            if group == 0:
                arrived[pl.ds(0, CAP), cols] = block[:CAP]
            return carry

        lax.fori_loop(0, 4, place_columns, 0)
        if group < 2:
            for p in range(max(1, group * 4), group * 4 + 4):
                disp_copy(p).start()

    loads["plane"].wait()
    for dz in (4, 3, 5, 2, 6, 1, 7):
        z_copy(dz).start()
    plane_pushes[0].start()
    with phase("one_1"):
        arrivals(1, *set_one)
    loads["d1"].wait()
    first_sends(*both("d1"))
    push("d1", 0)

    route = route_ref[...]
    slot_rows = lax.broadcasted_iota(jnp.int32, (EXPERTS * CAP, tokens), 0)
    weighted = jnp.where(slot_rows == slots[0], route[0:1, :], 0.0) + jnp.where(
        slot_rows == slots[1], route[1:2, :], 0.0
    )
    picking[...] = weighted.T.astype(jnp.bfloat16)

    with phase("halo"):
        halo_copy.wait_recv()
    row_count = pool_in.shape[1]
    window_group = (tp * 64) // GROUP_CH
    gain_wide = pool_gain[...]
    diagonal = lax.broadcasted_iota(jnp.int32, (64, 64), 0) == lax.broadcasted_iota(
        jnp.int32, (64, 64), 1
    )
    gain_col = jnp.sum(jnp.where(diagonal, gain_wide, 0.0), axis=1, keepdims=True)
    for part in range(4):
        r = slice(part * 16, part * 16 + 16)
        values = pool_in[r, :].astype(jnp.float32)
        carried = jnp.where(ep > 0, halo[r, :].astype(jnp.float32), 0.0)
        level = jnp.concatenate([carried, values], axis=1)
        summed = jnp.zeros_like(values)
        for doubling in range(4):
            level = level + pltpu.roll(level, 2**doubling, 1)
            summed = jnp.where(window_group == doubling, level[:, 128:], summed)
        position = ep * row_count + lax.broadcasted_iota(jnp.int32, (1, row_count), 1)
        width = 2 ** 1
        for doubling in range(1, 4):
            width = jnp.where(window_group == doubling, 2 ** (doubling + 1), width)
        counted = jnp.minimum(position + 1, width).astype(jnp.float32)
        pooled[r, :] = ((summed / counted - values) * gain_col[r, :]).astype(jnp.bfloat16)
    pooled_all[pl.ds(0, 64), :] = pooled[:, pl.ds(pl.multiple_of(tp * 128, 128), 128)]

    def pool_copy(dz, dc):
        target = lax.rem(pz + dz, NZ) * 2 + lax.rem(core + dc, 2)
        rel = -dz if dz <= 4 else NZ - dz
        return pltpu.make_async_remote_copy(
            src_ref=pooled.at[:, pl.ds(pl.multiple_of(target * 128, 128), 128)],
            dst_ref=pooled_all.at[pl.ds(SLOT_OF[rel] * 128 + 64 * dc, 64)],
            send_sem=pool_sem.at[0],
            recv_sem=pool_sem.at[1],
            device_id=column(dz, dc),
            device_id_type=DEV,
        )

    half_rows = 8 * CAP

    def gated(both_parts):
        gate_part, upward = both_parts[:, :128], both_parts[:, 128:]
        return (gate_part / (1.0 + jnp.exp(-gate_part)) * upward).astype(jnp.bfloat16)

    def project(rows, weights):
        return lax.dot_general(
            arrived[rows, :], weights, (((1,), (1,)), ((), ())), preferred_element_type=jnp.float32
        )

    def hidden_pairs(half, first_slot, pairs):
        rows = pl.ds(half * half_rows, half_rows)

        def one(pair, carry):
            slot = first_slot + 2 * pair
            sums = project(rows, w_in[pl.ds(slot, 2)].reshape(512, w_in.shape[2]))
            for k in range(2):
                cols = pl.ds(pl.multiple_of((slot + k) * 128, 128), 128)
                hidden[rows, cols] = gated(sums[:, 256 * k : 256 * k + 256])
            return carry

        lax.fori_loop(0, pairs, one, 0)

    def ret_copy(q, p):
        dx, dy = OFFSETS[p]
        rows = pl.ds(p * CAP, CAP)
        return pltpu.make_async_remote_copy(
            src_ref=rows_out.at[q, rows],
            dst_ref=rows_back.at[q, rows],
            send_sem=ret_send.at[q],
            recv_sem=ret_recv.at[q],
            device_id=plane(NX - dx, NY - dy),
            device_id_type=DEV,
        )

    def give_back(q, half):
        rows = pl.ds(half * half_rows, half_rows)
        block = jnp.dot(
            hidden[rows, :], w_down[q], preferred_element_type=jnp.float32
        ).astype(jnp.bfloat16)
        rows_out[q, rows] = block
        if half == 0:
            rows_back[q, pl.ds(0, CAP)] = block[:CAP]
        for p in range(max(1, half * 8), half * 8 + 8):
            ret_copy(q, p).start()

    def combine(q):
        wait_for(rows_back.at[q, pl.ds(CAP, 15 * CAP)], ret_recv.at[q])
        moe_ref[:, pl.ds(q * 512, 512)] = jnp.dot(
            picking[...], rows_back[q], preferred_element_type=jnp.float32
        ).astype(jnp.bfloat16)

    def down_ready(q):
        wait_for(w_down.at[q, pl.ds(0, 512)], sib_down.at[q])

    def in_ready(hop):
        for part in range(2):
            if hop == 1:
                wait_for(arrived.at[pl.ds(0, 192)], sib_in.at[part, 0])
            else:
                wait_for(w_in.at[0, pl.ds(0, 64 if hop == 4 else 128)], sib_in.at[part, hop - 1])

    with phase("in_1"):
        in_ready(1)
    for p in range(8, 16):
        disp_copy(p).start()
    with phase("one_2a"):
        arrivals(2, *set_one[:2])
    with phase("plane_z"):
        wait_for(z_bytes, plane_recv.at[0])
    for copy in x_copies:
        copy.start()
    with phase("one_2b"):
        arrivals(2, *set_one[2:])
    with phase("disp_0"):
        wait_for(arrived.at[pl.ds(CAP, 7 * CAP)], disp_recv.at[0])
        in_ready(2)
    with phase("hid_a"):
        hidden_pairs(0, 0, 2)
    with phase("one_3a"):
        arrivals(3, *set_one[:2])
    with phase("plane_x"):
        for copy in x_copies:
            copy.wait_recv()
    for copy in y_copies:
        copy.start()
    with phase("one_3b"):
        arrivals(3, *set_one[2:])
    with phase("d1_1"):
        arrivals(1, *both("d1"))
    for q in (2, 3):
        loads[f"d{q}"].wait()
    first_sends(*both("d2"))
    push("d2", 0)
    push("d3", 0)
    with phase("in_3"):
        in_ready(3)
    with phase("hid_b"):
        hidden_pairs(0, 4, 1)
    with phase("disp_1"):
        wait_for(arrived.at[pl.ds(8 * CAP, 8 * CAP)], disp_recv.at[1])
    with phase("hid_c"):
        hidden_pairs(1, 0, 3)
    with phase("one_4"):
        for half in range(2):
            for name in "gu":
                last_copy(name, half).wait_recv()
                push(name, SLOT_OF[4], pl.ds(32 * half, 32))
    with phase("one_4d"):
        arrivals(4, *set_one[4:])
    with phase("in_4"):
        in_ready(4)
    with phase("hid_67a"):
        hidden_pairs(0, 6, 1)
    with phase("d0"):
        down_ready(0)
    with phase("give_0a"):
        give_back(0, 0)
    with phase("d1_2"):
        arrivals(2, *both("d1"))
    first_sends(*both("d3"))
    with phase("hid_67b"):
        hidden_pairs(1, 6, 1)
    with phase("give_0b"):
        give_back(0, 1)
    with phase("d2_1"):
        arrivals(1, *both("d2"))
    with phase("d1_3"):
        arrivals(3, *both("d1"))
    with phase("d3_1"):
        arrivals(1, *both("d3"))
    with phase("d2_2"):
        arrivals(2, *both("d2"))
    with phase("d1_4"):
        arrivals(4, *both("d1"))
        down_ready(1)
    with phase("give_1a"):
        give_back(1, 0)
    with phase("two_2b"):
        arrivals(2, *both("d3"))
    for copy in y_copies:
        copy.wait_recv()
    plane_pushes[1].start()
    with phase("give_1b"):
        give_back(1, 1)
    with phase("two_3"):
        arrivals(3, *both("d2"))
    for h in range(2):
        loads[f"m{h}"].wait()
    with phase("two_3b"):
        arrivals(3, *both("d3"))
    first_sends(*set_mix)
    for h in range(2):
        push(f"m{h}", 0)
    for dz in (4, 3, 5, 2, 6, 1, 7, 0):
        for dc in range(2):
            if (dz, dc) != (0, 0):
                pool_copy(dz, dc).start()
    with phase("two_4"):
        arrivals(4, *both("d2"))
        arrivals(4, *both("d3"))
    with phase("d2"):
        down_ready(2)
    with phase("give_2"):
        give_back(2, 0)
        give_back(2, 1)
    with phase("d3"):
        down_ready(3)
    with phase("give_3"):
        give_back(3, 0)
        give_back(3, 1)
    with phase("mix_1"):
        arrivals(1, *set_mix)
    with phase("combine_0"):
        combine(0)
    with phase("mix_2"):
        arrivals(2, *set_mix)
    with phase("combine_1"):
        combine(1)
    with phase("pool_wait"):
        wait_for(pooled_all.at[pl.ds(64, 960)], pool_sem.at[1])
    pooled_rows[...] = pooled_all[...].astype(jnp.float32).T.astype(jnp.bfloat16)
    with phase("mix_3"):
        arrivals(3, *set_mix)

    with phase("mixer_0"):
        for push_copy in plane_pushes:
            push_copy.wait_recv()
        for cols in (pl.ds(0, 512), pl.ds(512, 512)):
            mixed_ref[:, cols] = jnp.dot(
                pooled_rows[...],
                w_plane[:, :, cols].reshape(1024, 512),
                preferred_element_type=jnp.float32,
            ).astype(jnp.bfloat16)
    for h in range(2):
        wait_for(w_mix.at[h, pl.ds(0, 448)], sib_mix.at[h, 0])
    with phase("mixer"):
        for h in range(2):
            mixed_sum[h] = jnp.dot(
                pooled_rows[:, :896], w_mix[h, :896], preferred_element_type=jnp.float32
            )
    with phase("combine_2"):
        combine(2)
    with phase("mix_4"):
        arrivals(4, *set_mix)
        for h in range(2):
            wait_for(w_mix.at[h, pl.ds(0, 64)], sib_mix.at[h, 1])
    with phase("mixer_2"):
        for h in range(2):
            last = jnp.dot(pooled_rows[:, 896:], w_mix[h, 896:], preferred_element_type=jnp.float32)
            mixed_ref[:, pl.ds(1024 + h * 512, 512)] = (mixed_sum[h] + last).astype(jnp.bfloat16)
    for name in names:
        if name in "gu":
            sent, pushed = outgoing.at[pl.ds(0, 7 * 64)], outgoing.at[pl.ds(0, 8 * 64)]
        else:
            whole = w_down.at[int(name[1])] if name[0] == "d" else w_mix.at[int(name[1])]
            sent, pushed = whole.at[pl.ds(0, 7 * 64)], whole.at[pl.ds(0, 8 * 64)]
        wait_for(sent, ring_send.at[number[name]])
        wait_for(pushed, push_send.at[number[name]])
    wait_for(outgoing.at[pl.ds(CAP, 15 * CAP)], disp_send)
    halo_copy.wait_send()
    wait_for(z_bytes, plane_send.at[0])
    for copy in (*x_copies, *y_copies, *plane_pushes):
        copy.wait_send()
    wait_for(pooled_all.at[pl.ds(64, 960)], pool_sem.at[0])
    for q in range(3):
        wait_for(rows_out.at[q, pl.ds(CAP, 15 * CAP)], ret_send.at[q])
    with phase("combine_3"):
        combine(3)
    with phase("end"):
        wait_for(rows_out.at[3, pl.ds(CAP, 15 * CAP)], ret_send.at[3])


def store_kernel(mixed_ref, moe_ref, mixed_hbm, moe_hbm, sems):
    copies = []
    for source, target, parts in ((moe_ref, moe_hbm, 4), (mixed_ref, mixed_hbm, 2)):
        rows = source.shape[0] // parts
        for k in range(parts):
            part = pl.ds(k * rows, rows)
            copies.append(
                pltpu.make_async_copy(source.at[part], target.at[part], sems.at[len(copies)])
            )
    for copy in copies:
        copy.start()
    for copy in copies:
        copy.wait()


def body(
    pool_input,
    pool_gain,
    mix_weight,
    moe_input,
    moe_gain,
    expert_ids,
    route_weight,
    gate_weight,
    up_weight,
    down_weight,
):
    rows_a, channels = pool_input.shape
    tokens, width = moe_input.shape
    slots = EXPERTS * CAP
    bf, f32 = jnp.bfloat16, jnp.float32
    hbm = pl.BlockSpec(memory_space=pl.ANY)
    vmem = pl.BlockSpec(memory_space=pltpu.VMEM)
    dma = pltpu.SemaphoreType.DMA
    mixed, moe = pl.pallas_call(
        kernel,
        out_shape=(
            pltpu.VMEM((rows_a // 16, width), bf),
            pltpu.VMEM((tokens, width), bf),
        ),
        in_specs=[hbm] * 10,
        out_specs=(vmem, vmem),
        scratch_shapes=[
            pltpu.VMEM((8, 256, width), bf),
            pltpu.VMEM((4, 1024, 512), bf),
            pltpu.VMEM((2, 1024, 512), bf),
            pltpu.VMEM((8, 128, 1024), bf),
            pltpu.VMEM((channels, rows_a), bf),
            pltpu.VMEM((channels, 128), bf),
            pltpu.VMEM((channels, rows_a), bf),
            pltpu.VMEM((1024, 128), bf),
            pltpu.VMEM((tokens, width), bf),
            pltpu.VMEM((tokens, width), bf),
            pltpu.VMEM((4 * CAP, tokens), bf),
            pltpu.VMEM((tokens, slots), bf),
            pltpu.VMEM((slots, width), bf),
            pltpu.VMEM((slots, width), bf),
            pltpu.VMEM((slots, 1024), bf),
            pltpu.VMEM((4, slots, 512), bf),
            pltpu.VMEM((4, slots, 512), bf),
            pltpu.VMEM((rows_a // 16, 1024), bf),
            pltpu.VMEM((2, rows_a // 16, 512), f32),
            pltpu.VMEM((1, channels), f32),
            pltpu.VMEM((1, width), f32),
            pltpu.VMEM((2, tokens), jnp.int32),
            pltpu.VMEM((2, tokens), f32),
            dma((15,)),
            dma((8, 8)),
            dma((8,)),
            dma((8,)),
            dma((2, 4)),
            dma((4,)),
            dma((2, 2)),
            dma((11,)),
            dma((11,)),
            dma,
            dma((2,)),
            dma((2,)),
            dma((2,)),
            dma((4,)),
            dma((4,)),
        ],
        compiler_params=pltpu.CompilerParams(
            collective_id=0, has_side_effects=True, vmem_limit_bytes=56 << 20
        ),
        name="mixer_and_experts",
    )(
        gate_weight[0].T,
        up_weight[0].T,
        down_weight[0].T,
        mix_weight,
        pool_input.T,
        moe_input,
        pool_gain.reshape(1, channels),
        moe_gain.reshape(1, width),
        expert_ids.T,
        route_weight.T,
    )
    return pl.pallas_call(
        store_kernel,
        out_shape=(
            jax.ShapeDtypeStruct(mixed.shape, bf),
            jax.ShapeDtypeStruct(moe.shape, bf),
        ),
        in_specs=(vmem, vmem),
        out_specs=(hbm, hbm),
        scratch_shapes=[dma((6,))],
        name="store",
    )(*(pltpu.with_memory_space_constraint(a, pltpu.VMEM) for a in (mixed, moe)))


def solution(mesh):
    return jax.shard_map(
        body,
        mesh=mesh,
        in_specs=(
            P("ep", "tp"),
            P("tp"),
            P("tp", None),
            P(("ep", "tp"), None),
            P(),
            P(("ep", "tp"), None),
            P(("ep", "tp"), None),
            P("ep", None, "tp"),
            P("ep", None, "tp"),
            P("ep", None, "tp"),
        ),
        out_specs=(P(("ep", "tp"), None), P(("ep", "tp"), None)),
        check_vma=False,
    )
```
